256 devices in a mesh: sp: 16 (over y, x), tp: 16 (over z, core).
Axes of the slice: x: 4, y: 4, z: 8, core: 2. Of those that a mesh axis runs over, the one named last changes fastest.
Arguments:
- residual: bfloat16 [4096, 2048], P(('sp', 'tp')), may hold values from -6 to 6
- mixer_in: bfloat16 [4096, 2048], P('sp', 'tp'), may hold values from -6 to 6
- doc_ids: int32 [4096], P('sp'), may hold values from 0 to 3, never falling along the last dimension, each value on 1 to 1536 neighbouring positions
- lam_re: float32 [128, 64], P('tp'), may hold values from -1 to 0, as said below
- lam_im: float32 [128, 64], P('tp'), may hold values from 0 to 256
- log_step: float32 [128], P('tp'), may hold values from -3 to -2
- log_keep: float32 [4096, 128], P('sp', 'tp'), may hold values from -1.5 to 0, as said below
- in_re: float32 [128, 64, 16], P('tp'), may hold values from -1 to 1
- in_im: float32 [128, 64, 16], P('tp'), may hold values from -1 to 1
- out_re: float32 [128, 16, 64], P('tp'), may hold values from -0.5 to 0.5
- out_im: float32 [128, 16, 64], P('tp'), may hold values from -0.5 to 0.5
- skip_gain: float32 [2048], P('tp'), may hold values from -4 to 4
- w_val: bfloat16 [2048, 2048], P('tp'), may hold values from -0.125 to 0.125
- w_gate: bfloat16 [2048, 2048], P('tp'), may hold values from -0.125 to 0.125
- norm_gain: float32 [2048], replicated, may hold values from 0.1 to 1.9
- route_ids: int32 [4096, 2], P('sp'), may hold values from 0 to 15, all different within a row; in each aligned block of 16 rows (0 to 15, 16 to 31, ...) at most 2 rows name the same one
- route_wts: float32 [4096, 2], P('sp'), may hold values from 0.2 to 1.5
- exp_gate: bfloat16 [16, 2048, 4096], P('sp', None, 'tp'), may hold values from -0.125 to 0.125
- exp_up: bfloat16 [16, 2048, 4096], P('sp', None, 'tp'), may hold values from -0.125 to 0.125
- exp_down: bfloat16 [16, 4096, 2048], P('sp', 'tp'), may hold values from -0.09375 to 0.09375
- shared_gate: bfloat16 [2048, 512], replicated, may hold values from -0.125 to 0.125
- shared_up: bfloat16 [2048, 512], replicated, may hold values from -0.125 to 0.125
- shared_down: bfloat16 [512, 2048], replicated, may hold values from -0.25 to 0.25
Outputs:
- mixed: bfloat16 [4096, 2048], P(('sp', 'tp'))
The draws below stay inside these ranges and needn't reach their ends.
Inputs may be any that keep to these rules, and one draw needn't show every extreme that they name: `doc_ids`: document numbers start at 0 and never fall; each document has 1 to 1536 positions. `route_ids`: in each aligned block of 16 positions (the positions of one device after the mixer), no expert is named more than 2 times, and some block names one expert exactly 2 times; a position names 2 different experts. `lam_re`: Negative. `log_keep`: never positive.
All inputs are finite; a program needn't handle non-finite values.
Results may differ from the reference program's by a relative error of at most 0.017.
Values may be sent and summed in bfloat16 or wider, within the bound.
No kernel may reach another device: no remote copies, remote signals or barrier semaphores. Data moves between devices by JAX's collectives and lax.ppermute only.
A program may use at most 64 MiB of HBM per device.

```python
import math
import jax
import jax.numpy as jnp
import numpy as np
from jax import lax

D = 2048
GROUP = 16
GROUPS = 128
STATE = 64
EFF = 4096
SFF = 512
EXPERTS = 16
TOP = 2
S_DEV = 256
TOKEN_POSITIONS = 4096
TOK_LOC = 16
CAP = 2
DOCS = 4
DOC_MOST = 1536
N_SP = 16
N_TP = 16


def decay_parts(key):
    random_subkeys = jax.random.split(jax.random.fold_in(key, 11), 4)
    fast_draw = jax.random.randint(random_subkeys[0], (GROUPS,), 0, 2)
    is_fast = fast_draw == 0
    time_step = jnp.exp(jax.random.uniform(random_subkeys[1], (GROUPS,), jnp.float32, math.log(0.05), math.log(0.1)))
    fast_rate = jnp.exp(jax.random.uniform(random_subkeys[2], (GROUPS, STATE), jnp.float32, math.log(1.0 / 50), math.log(1.0 / 30)))
    slow_rate = jax.random.uniform(random_subkeys[3], (GROUPS, STATE), jnp.float32, 0.2, 0.5) / TOKEN_POSITIONS
    decay_rate = jnp.where(is_fast[:, None], fast_rate, slow_rate)
    return (-decay_rate / time_step[:, None], jnp.log(time_step))


def draw_lam_re(key, part):
    return decay_parts(key)[0]


def draw_log_step(key, part):
    return decay_parts(key)[1]


def draw_lam_im(key, part):
    jitter = jax.random.uniform(jax.random.fold_in(key, 17), (GROUPS, STATE), jnp.float32, 0.3, 1.0)
    return math.pi * jnp.arange(STATE, dtype=jnp.float32)[None, :] + jitter


def draw_log_keep(key, part):
    random_subkeys = jax.random.split(jax.random.fold_in(key, 23), 3)
    spans = TOKEN_POSITIONS // S_DEV
    extra = jax.random.uniform(random_subkeys[0], (spans, GROUPS), jnp.float32, 0.0, 1.2) / TOKEN_POSITIONS
    slope = jnp.repeat(extra, S_DEV, axis=0)
    reset_position = jax.random.randint(random_subkeys[1], (8,), 0, TOKEN_POSITIONS)
    depth = jax.random.uniform(random_subkeys[2], (8, GROUPS), jnp.float32, math.log(0.5), math.log(0.8))
    match_flags = (jnp.arange(TOKEN_POSITIONS)[:, None] == reset_position[None, :]).astype(jnp.float32)
    return jnp.dot(match_flags, depth, precision=lax.Precision.HIGHEST) - slope


def steps_of(stream_key, dims, cuts, least, largest):
    def one(position, shards_of):
        heights = jax.random.uniform(jax.random.fold_in(jax.random.fold_in(stream_key, 6), position), (shards_of,), jnp.float32, least / len(cuts), largest / len(cuts))
        return jnp.repeat(jnp.exp(heights), dims[position] // shards_of).reshape((-1,) + (1,) * (len(dims) - position - 1))

    level = one(*cuts[0])
    for cut in cuts[1:]:
        level = level * one(*cut)
    return level


def profile(count, total, reach, skew):
    loads = [(1 << 20) // math.isqrt(standing ** skew) + 1 for standing in range(2, count + 1)]
    surplus, counts = total - reach - (count - 1), [1] * (count - 1)
    while surplus > 0:
        candidates = [i for i in range(count - 1) if counts[i] < reach]
        pool, left = sum([loads[i] for i in candidates]), surplus
        for i in candidates:
            addition = min(reach - counts[i], max(1, left * loads[i] // pool), surplus)
            counts[i] = counts[i] + addition
            surplus = surplus - addition
    return np.array([reach] + counts)


def uneven_parts(key, number_of, total, limit, skew):
    if number_of == 2:
        one = jax.random.randint(key, (), max(1, total - limit), min(limit, total - 1) + 1)
        return jnp.stack([one, total - one])
    lengths = jnp.asarray(profile(number_of, total, limit, skew), jnp.int32)
    twos = (number_of - 1) // 2
    donor, taker = lengths[1:1 + 2 * twos:2], lengths[2:2 + 2 * twos:2]
    room = jnp.minimum(donor - 1, limit - taker)
    shifted = jax.random.randint(jax.random.fold_in(key, 1), (twos,), 0, 1 << 20) % (room + 1)
    lengths = lengths.at[1:1 + 2 * twos:2].set(donor - shifted).at[2:2 + 2 * twos:2].set(taker + shifted)
    return lengths[jax.random.permutation(jax.random.fold_in(key, 2), number_of)]


def assign_block(key, own, number, rows, number_of, top, reach, skew):
    sequence = jax.random.permutation(key, number_of)
    packed, usual = shares(number_of, rows * top, reach, skew, True), shares(number_of, rows * top, reach, skew, False)
    places = jnp.arange(number_of)

    def named(sizes, offset_by):
        used = int((sizes > 0).sum())
        fixed = max(1, used // 4)
        moved = fixed + (places - fixed + offset_by * (used - fixed)) % max(1, number_of - fixed)
        return jnp.zeros((number_of,), jnp.int32).at[sequence[jnp.where(places < fixed, places, moved)]].set(jnp.asarray(sizes, jnp.int32))

    sizes = jnp.where(number % 4 == 0, named(packed, number // 4), named(usual, number - number // 4 - 1))
    mixed = jax.random.permutation(jax.random.fold_in(own, 3), number_of)
    giver, taker = mixed[0:number_of // 2 * 2:2], mixed[1:number_of // 2 * 2:2]
    room = jnp.minimum(sizes[giver] - 1, reach - sizes[taker]) // 2
    room = jnp.where((giver == sequence[0]) | (taker == sequence[0]) | (sizes[taker] == 0), 0, jnp.maximum(room, 0))
    moved = jax.random.randint(jax.random.fold_in(own, 4), (number_of // 2,), 0, 1 << 20) % (room + 1)
    sizes = sizes.at[giver].add(-moved).at[taker].add(moved)
    members = jnp.searchsorted(jnp.cumsum(sizes), jnp.arange(rows * top), side="right").astype(jnp.int32)
    table = members.reshape(top, rows).T
    table = table[jax.random.permutation(jax.random.fold_in(own, 1), rows)]
    offset_by = jax.random.randint(jax.random.fold_in(own, 2), (rows, 1), 0, top)
    return jnp.take_along_axis(table, (jnp.arange(top)[None, :] + offset_by) % top, axis=1)


def shares(number_of, total, most, skew, full):
    loads = [(1 << 20) // math.isqrt(rank ** skew) + 1 for rank in range(1, number_of + 1)]
    largest = most if full else min(most, max(-(-total // number_of), total * loads[0] // sum(loads)))
    least = 1 if total - largest >= number_of - 1 else 0
    holding, rest = [largest] + [least] * (number_of - 1), total - largest - least * (number_of - 1)
    while rest > 0:
        movable = [i for i in range(1, number_of) if holding[i] < largest] or [i for i in range(1, number_of) if holding[i] < most]
        whole, budget = sum([loads[i] for i in movable]), rest
        for i in movable:
            more = min(most - holding[i], max(1, budget * loads[i] // whole), rest)
            holding[i] = holding[i] + more
            rest = rest - more
    return np.array(holding)


def gaussian(own_key, shape, width, reach, shards=(), held_as=jnp.bfloat16):
    values = width * jax.random.normal(own_key, shape, jnp.float32)
    if shards:
        values = values * steps_of(own_key, shape, shards, -0.22, 0.18)
    return jnp.clip(values, -reach, reach).astype(held_as)


def setup_inputs(seed: int = 0) -> dict:
    seeds = jax.random.split(jax.random.key(seed), 24)
    residual = gaussian(seeds[0], (TOKEN_POSITIONS, D), 1.0, 6.0, ((0, 256),))
    mixer_in = gaussian(seeds[1], (TOKEN_POSITIONS, D), 1.0, 6.0, ((0, 16), (1, 16)))
    doc_ids = jnp.searchsorted(jnp.cumsum(uneven_parts(seeds[2], DOCS, TOKEN_POSITIONS, DOC_MOST, 0)), jnp.arange(TOKEN_POSITIONS), side="right").astype(jnp.int32)
    lam_re = draw_lam_re(jax.random.fold_in(seeds[23], 71), 0)
    lam_im = draw_lam_im(jax.random.fold_in(seeds[23], 71), 0)
    log_step = draw_log_step(jax.random.fold_in(seeds[23], 71), 0)
    log_keep = draw_log_keep(jax.random.fold_in(seeds[23], 71), 0)
    in_re = gaussian(seeds[7], (GROUPS, STATE, GROUP), (2 * GROUP) ** -0.5, 1.0, ((0, 16),), jnp.float32)
    in_im = gaussian(seeds[8], (GROUPS, STATE, GROUP), (2 * GROUP) ** -0.5, 1.0, ((0, 16),), jnp.float32)
    out_re = gaussian(seeds[9], (GROUPS, GROUP, STATE), (2 * STATE) ** -0.5, 0.5, ((0, 16),), jnp.float32)
    out_im = gaussian(seeds[10], (GROUPS, GROUP, STATE), (2 * STATE) ** -0.5, 0.5, ((0, 16),), jnp.float32)
    skip_gain = gaussian(seeds[11], (D,), 1.0, 4.0, ((0, 16),), jnp.float32)
    w_val = gaussian(seeds[12], (D, D), D ** -0.5, 0.125, ((0, 16),))
    w_gate = gaussian(seeds[13], (D, D), D ** -0.5, 0.125, ((0, 16),))
    norm_gain = jnp.clip(1.0 + 0.18 * jax.random.normal(seeds[14], (D,), jnp.float32), 0.1, 1.9)
    route_ids_keys = jax.random.split(jax.random.fold_in(seeds[15], 1), TOKEN_POSITIONS // TOK_LOC)
    route_ids_turns = jax.random.permutation(jax.random.fold_in(seeds[15], 3), TOKEN_POSITIONS // TOK_LOC)
    route_ids = jax.vmap(lambda own, number: assign_block(jax.random.fold_in(seeds[15], 2), own, number, TOK_LOC, EXPERTS, TOP, CAP, 2))(route_ids_keys, route_ids_turns).reshape((TOKEN_POSITIONS, TOP))
    route_wts = jnp.clip(0.2 + 1.3 * jax.random.uniform(seeds[16], (TOKEN_POSITIONS, TOP), jnp.float32) ** steps_of(seeds[16], (TOKEN_POSITIONS, TOP), ((0, 16),), -0.2, 0.2), 0.2, 1.5)
    exp_gate = gaussian(seeds[17], (EXPERTS, D, EFF), D ** -0.5, 0.125, ((0, 16), (2, 16)))
    exp_up = gaussian(seeds[18], (EXPERTS, D, EFF), D ** -0.5, 0.125, ((0, 16), (2, 16)))
    exp_down = gaussian(seeds[19], (EXPERTS, EFF, D), EFF ** -0.5, 0.09375, ((0, 16), (1, 16)))
    shared_gate = gaussian(seeds[20], (D, SFF), D ** -0.5, 0.125)
    shared_up = gaussian(seeds[21], (D, SFF), D ** -0.5, 0.125)
    shared_down = gaussian(seeds[22], (SFF, D), SFF ** -0.5, 0.25)
    return dict(residual=residual, mixer_in=mixer_in, doc_ids=doc_ids, lam_re=lam_re, lam_im=lam_im, log_step=log_step, log_keep=log_keep, in_re=in_re, in_im=in_im, out_re=out_re, out_im=out_im, skip_gain=skip_gain, w_val=w_val, w_gate=w_gate, norm_gain=norm_gain, route_ids=route_ids, route_wts=route_wts, exp_gate=exp_gate, exp_up=exp_up, exp_down=exp_down, shared_gate=shared_gate, shared_up=shared_up, shared_down=shared_down)


HIGHEST = lax.Precision.HIGHEST
EPSILON = 1e-06

def complex_join(earlier, latter):
    return (earlier[0] * latter[0] - earlier[1] * latter[1], earlier[0] * latter[1] + earlier[1] * latter[0], latter[0] * earlier[2] - latter[1] * earlier[3] + latter[2], latter[0] * earlier[3] + latter[1] * earlier[2] + latter[3])

def input_map(lam_re, lam_im, log_step, in_re, in_im):
    time_step = jnp.exp(log_step)[:, None]
    magnitude = jnp.exp(lam_re * time_step)
    minus_re = magnitude * jnp.cos(lam_im * time_step) - 1.0
    minus_im = magnitude * jnp.sin(lam_im * time_step)
    denom = lam_re * lam_re + lam_im * lam_im
    quot_re = (minus_re * lam_re + minus_im * lam_im) / denom
    quot_im = (minus_im * lam_re - minus_re * lam_im) / denom
    bar_re = quot_re[..., None] * in_re - quot_im[..., None] * in_im
    bar_im = quot_re[..., None] * in_im + quot_im[..., None] * in_re
    return (bar_re, bar_im)

def state_mixer(mixer_in, doc_ids, lam_re, lam_im, log_step, log_keep, in_re, in_im, out_re, out_im, skip_gain):
    total_rows = mixer_in.shape[0]
    groups = lam_re.shape[0]
    inputs = mixer_in.astype(jnp.float32).reshape(total_rows, groups, -1)
    bar_re, bar_im = input_map(lam_re, lam_im, log_step, in_re, in_im)
    time_step = jnp.exp(log_step)[:, None]
    turn_angle = lam_im * time_step
    previous = jnp.concatenate([doc_ids[:1], doc_ids[:-1]])
    alive = (doc_ids == previous).astype(jnp.float32)
    span_rows = 512
    blocks = total_rows // span_rows

    def one_block(carried, stacked):
        block_in, retention_logarithm, living_block = stacked
        drive_re = jnp.einsum('sgh,gph->sgp', block_in, bar_re, precision=HIGHEST)
        drive_im = jnp.einsum('sgh,gph->sgp', block_in, bar_im, precision=HIGHEST)
        magnitude = jnp.exp(lam_re * time_step + retention_logarithm[:, :, None]) * living_block[:, None, None]
        dec_re = magnitude * jnp.cos(turn_angle)
        dec_im = magnitude * jnp.sin(turn_angle)
        cum_re, cum_im, loc_re, loc_im = lax.associative_scan(complex_join, (dec_re, dec_im, drive_re, drive_im), axis=0)
        carry_re, carry_im = carried
        state_re = loc_re + cum_re * carry_re - cum_im * carry_im
        state_imaginary = loc_im + cum_re * carry_im + cum_im * carry_re
        readout = jnp.einsum('sgp,ghp->sgh', state_re, out_re, precision=HIGHEST) - jnp.einsum('sgp,ghp->sgh', state_imaginary, out_im, precision=HIGHEST)
        return ((state_re[-1], state_imaginary[-1]), readout)
    stacked = (inputs.reshape(blocks, span_rows, groups, -1), log_keep.reshape(blocks, span_rows, groups), alive.reshape(blocks, span_rows))
    empty_state = jnp.zeros(lam_re.shape, jnp.float32)
    _, readout = lax.scan(one_block, (empty_state, empty_state), stacked)
    readout = readout.reshape(total_rows, -1) + skip_gain * mixer_in.astype(jnp.float32)
    return jax.nn.gelu(readout).astype(jnp.bfloat16)

def glu_sums(activation, w_val, w_gate):
    total_rows, model_width = activation.shape
    block_width = model_width // N_TP
    stacked = jnp.concatenate([w_val, w_gate], axis=1)

    def add_block(running, block_index):
        part_act = lax.dynamic_slice_in_dim(activation, block_index * block_width, block_width, 1)
        part_rows = lax.dynamic_slice_in_dim(stacked, block_index * block_width, block_width, 0)
        partial_out = jnp.dot(part_act, part_rows, preferred_element_type=jnp.float32).astype(jnp.bfloat16)
        partial_out = lax.optimization_barrier(partial_out)
        return (running + partial_out.astype(jnp.float32), None)
    summed, _ = lax.scan(add_block, jnp.zeros((total_rows, stacked.shape[1]), jnp.float32), jnp.arange(N_TP))
    return (summed[:, :model_width], summed[:, model_width:])

def routed_experts(normed, route_ids, route_wts, exp_gate, exp_up, exp_down):
    total_rows, model_width = normed.shape
    top_k = route_ids.shape[1]
    expert_count = exp_gate.shape[0]
    tok_loc = total_rows // (N_SP * N_TP)
    capacity = 5 * tok_loc * top_k // (4 * expert_count)
    most_rows = N_SP * N_TP * capacity
    block_width = exp_down.shape[1] // N_TP
    flat_ids = route_ids.reshape(-1)
    pad_wts = jnp.concatenate([route_wts.reshape(-1), jnp.zeros((1,), jnp.float32)])
    padded = jnp.concatenate([normed, jnp.zeros((1, model_width), normed.dtype)], axis=0)

    def one_expert(routed_tokens, expert):
        places = jnp.nonzero(flat_ids == expert, size=most_rows, fill_value=total_rows * top_k)[0].astype(jnp.int32)
        owners = (places // top_k).astype(jnp.int32)
        gathered = padded[owners]
        weights = pad_wts[places]
        gate_pre = jnp.dot(gathered, exp_gate[expert], preferred_element_type=jnp.float32)
        up_pre = jnp.dot(gathered, exp_up[expert], preferred_element_type=jnp.float32)
        inner_act = (jax.nn.silu(gate_pre) * up_pre).astype(jnp.bfloat16)

        def add_block(running, block_index):
            part_act = lax.dynamic_slice_in_dim(inner_act, block_index * block_width, block_width, 1)
            down_rows = lax.dynamic_slice_in_dim(exp_down[expert], block_index * block_width, block_width, 0)
            partial_out = jnp.dot(part_act, down_rows, preferred_element_type=jnp.float32).astype(jnp.bfloat16)
            partial_out = lax.optimization_barrier(partial_out)
            return (running + partial_out.astype(jnp.float32), None)
        summed, _ = lax.scan(add_block, jnp.zeros((most_rows, model_width), jnp.float32), jnp.arange(N_TP))
        rounded = lax.optimization_barrier(summed.astype(jnp.bfloat16))
        output = rounded.astype(jnp.float32) * weights[:, None]
        return (routed_tokens.at[owners].add(output), None)
    routed_tokens, _ = lax.scan(one_expert, jnp.zeros((total_rows + 1, model_width), jnp.float32), jnp.arange(expert_count))
    return routed_tokens[:total_rows]

def reference(residual, mixer_in, doc_ids, lam_re, lam_im, log_step, log_keep, in_re, in_im, out_re, out_im, skip_gain, w_val, w_gate, norm_gain, route_ids, route_wts, exp_gate, exp_up, exp_down, shared_gate, shared_up, shared_down):
    activation = state_mixer(mixer_in, doc_ids, lam_re, lam_im, log_step, log_keep, in_re, in_im, out_re, out_im, skip_gain)
    value_pre, gate_pre = glu_sums(activation, w_val, w_gate)
    hidden = residual.astype(jnp.float32) + value_pre * jax.nn.sigmoid(gate_pre)
    normed = (hidden * lax.rsqrt(lax.optimization_barrier(jnp.mean(hidden * hidden, axis=-1, keepdims=True)) + EPSILON) * norm_gain).astype(jnp.bfloat16)
    routed_tokens = routed_experts(normed, route_ids, route_wts, exp_gate, exp_up, exp_down)
    shared_inner = (jax.nn.silu(jnp.dot(normed, shared_gate, preferred_element_type=jnp.float32)) * jnp.dot(normed, shared_up, preferred_element_type=jnp.float32)).astype(jnp.bfloat16)
    shared_out = jnp.dot(shared_inner, shared_down, preferred_element_type=jnp.float32)
    return (hidden + routed_tokens + shared_out).astype(jnp.bfloat16)
```

```python
import jax
import jax.numpy as jnp
from jax import lax
from jax.experimental import pallas as pl
from jax.experimental.pallas import tpu as pltpu
from jax.sharding import Mesh, PartitionSpec as P

EPSILON = 1e-06
SP = ("y", "x")
TP = ("z", "core")
STEPS = 32
CHUNKS = 8
LANES = 128
F32 = jnp.float32
BF16 = jnp.bfloat16


def halves(x):
    high = x.astype(BF16)
    return high, (x - high.astype(F32)).astype(BF16)


def dot_nt(a, b):
    return lax.dot_general(a, b, (((1,), (1,)), ((), ())), preferred_element_type=F32)


def block_rows(parts, group_states):
    groups, states = parts.shape
    tiled = jnp.concatenate([parts] * groups, axis=1)
    lane_group = lax.broadcasted_iota(jnp.int32, tiled.shape, 1) // states
    row = lax.broadcasted_iota(jnp.int32, tiled.shape, 0)
    return jnp.sum(jnp.where(lane_group == row, tiled, 0.0), axis=0, keepdims=True)


def decay_rows(lam_re, lam_im, log_step):
    time_step = jnp.exp(log_step)
    magnitude = jnp.exp(lam_re * time_step)
    angle = lam_im * time_step
    return magnitude * jnp.cos(angle), magnitude * jnp.sin(angle)


def squared(re, im, times):
    for _ in range(times):
        re, im = re * re - im * im, 2.0 * re * im
    return re, im


def store_lanes(ref, x):
    for i in range(ref.shape[0]):
        ref[i] = x[:, i * LANES : (i + 1) * LANES]


def strided(ref, j):
    at = pl.ds(j, CHUNKS, stride=STEPS)
    return jnp.concatenate([ref[i, at, :] for i in range(ref.shape[0])], axis=1)


def drive_kernel(
    u_ref, keep_ref, docs_ref, lam_re_ref, lam_im_ref, step_ref, in_re_ref, in_im_ref,
    send_ref, finals_ref, dre_ref, dim_ref, kx_ref, a_ref,
):
    lam_re, lam_im = lam_re_ref[...], lam_im_ref[...]
    groups, states = lam_re.shape
    width = groups * states
    dec_re, dec_im = decay_rows(lam_re, lam_im, step_ref[...])
    denom = lam_re * lam_re + lam_im * lam_im
    less = dec_re - 1.0
    quot_re = block_rows((less * lam_re + dec_im * lam_im) / denom, states)
    quot_im = block_rows((dec_im * lam_re - less * lam_im) / denom, states)
    a_re, a_im = block_rows(dec_re, states), block_rows(dec_im, states)
    a_ref[0:1, :], a_ref[1:2, :] = a_re, a_im
    u = u_ref[...]
    rows, channels = u.shape
    per_group = channels // groups
    row_group = lax.broadcasted_iota(jnp.int32, (width, channels), 0) // states
    lane_group = lax.broadcasted_iota(jnp.int32, (width, channels), 1) // per_group
    own = row_group == lane_group

    def spread(ref):
        tiled = jnp.where(own, jnp.concatenate([ref[...]] * groups, axis=1), 0.0)
        high, low = halves(tiled)
        return dot_nt(u, high) + dot_nt(u, low)

    raw_re, raw_im = spread(in_re_ref), spread(in_im_ref)
    store_lanes(dre_ref, quot_re * raw_re - quot_im * raw_im)
    store_lanes(dim_ref, quot_re * raw_im + quot_im * raw_re)
    expand = (
        lax.broadcasted_iota(jnp.int32, (groups, width), 1) // states
        == lax.broadcasted_iota(jnp.int32, (groups, width), 0)
    ).astype(F32)
    kept_wide = jnp.dot(
        keep_ref[...], expand, precision=lax.Precision.HIGHEST, preferred_element_type=F32
    )
    store_lanes(kx_ref, kept_wide)
    wide = (CHUNKS, width)
    ar, ai = jnp.broadcast_to(a_re, wide), jnp.broadcast_to(a_im, wide)
    s_re, s_im = jnp.zeros(wide, F32), jnp.zeros(wide, F32)
    total = jnp.ones(wide, F32)
    for j in range(STEPS):
        k = strided(kx_ref, j)
        s_re, s_im = (
            k * (ar * s_re - ai * s_im) + strided(dre_ref, j),
            k * (ar * s_im + ai * s_re) + strided(dim_ref, j),
        )
        total = total * k
    finals_ref[0], finals_ref[1], finals_ref[2] = s_re, s_im, total
    b_re, b_im = squared(a_re, a_im, 5)
    c_re, c_im, kept = s_re[0:1], s_im[0:1], total[0:1]
    for c in range(1, CHUNKS):
        k = total[c : c + 1]
        c_re, c_im = (
            k * (b_re * c_re - b_im * c_im) + s_re[c : c + 1],
            k * (b_re * c_im + b_im * c_re) + s_im[c : c + 1],
        )
        kept = kept * k
    packed = jnp.concatenate(
        [c_re, c_im, kept, jnp.broadcast_to(docs_ref[...], (1, width))], axis=0
    )
    send_ref[...] = jnp.broadcast_to(packed[None], send_ref.shape)


def readout_kernel(
    place_ref, got_ref, finals_ref, dre_ref, dim_ref, kx_ref, a_ref, u_ref, out_re_ref, out_im_ref,
    skip_ref, own_ref, other_ref, sre_ref, sim_ref,
):
    position, core = place_ref[0], place_ref[1]
    devices = got_ref.shape[0]
    width = a_ref.shape[1]
    a_re, a_im = a_ref[0:1, :], a_ref[1:2, :]
    b_re, b_im = squared(a_re, a_im, 5)
    w_re, w_im = squared(b_re, b_im, 3)
    c_re, c_im = jnp.zeros((1, width), F32), jnp.zeros((1, width), F32)
    closing = jnp.full((1, width), -1.0, F32)
    for i in range(devices):
        docs = got_ref[i, 3:4, :]
        last = jnp.floor(docs * 0.125)
        first = docs - 8.0 * last
        before = jnp.int32(i) < position
        here = jnp.int32(i) <= position
        linked = jnp.where(first == closing, 1.0, 0.0)
        c_re = jnp.where(here, linked * c_re, c_re)
        c_im = jnp.where(here, linked * c_im, c_im)
        k = got_ref[i, 2:3, :]
        n_re = k * (w_re * c_re - w_im * c_im) + got_ref[i, 0:1, :]
        n_im = k * (w_re * c_im + w_im * c_re) + got_ref[i, 1:2, :]
        c_re, c_im = jnp.where(before, n_re, c_re), jnp.where(before, n_im, c_im)
        closing = last
    heads_re, heads_im = [c_re], [c_im]
    for c in range(CHUNKS - 1):
        k = finals_ref[2, c : c + 1, :]
        c_re, c_im = (
            k * (b_re * c_re - b_im * c_im) + finals_ref[0, c : c + 1, :],
            k * (b_re * c_im + b_im * c_re) + finals_ref[1, c : c + 1, :],
        )
        heads_re.append(c_re)
        heads_im.append(c_im)
    s_re, s_im = jnp.concatenate(heads_re, axis=0), jnp.concatenate(heads_im, axis=0)
    wide = (CHUNKS, width)
    ar, ai = jnp.broadcast_to(a_re, wide), jnp.broadcast_to(a_im, wide)
    for j in range(STEPS):
        k = strided(kx_ref, j)
        s_re, s_im = (
            k * (ar * s_re - ai * s_im) + strided(dre_ref, j),
            k * (ar * s_im + ai * s_re) + strided(dim_ref, j),
        )
        for i in range(width // LANES):
            at = pl.ds(j, CHUNKS, stride=STEPS)
            sre_ref[i, at, :] = s_re[:, i * LANES : (i + 1) * LANES]
            sim_ref[i, at, :] = s_im[:, i * LANES : (i + 1) * LANES]
    rows, channels = u_ref.shape
    states = out_re_ref.shape[1]
    groups = width // states
    row_group = lax.broadcasted_iota(jnp.int32, (channels, width), 0) // (channels // groups)
    lane_group = lax.broadcasted_iota(jnp.int32, (channels, width), 1) // states
    own = row_group == lane_group

    def gathered(state_ref, ref):
        tiled = jnp.where(own, jnp.concatenate([ref[...]] * groups, axis=1), 0.0)
        high, low = halves(tiled)
        blocks = [state_ref[i] for i in range(width // LANES)]
        s_high, s_low = halves(jnp.concatenate(blocks, axis=1))
        return dot_nt(s_high, high) + dot_nt(s_high, low) + dot_nt(s_low, high)

    readout = gathered(sre_ref, out_re_ref) - gathered(sim_ref, out_im_ref)
    readout = readout + skip_ref[...] * u_ref[...].astype(F32)
    active = jax.nn.gelu(readout)
    tiles = active.reshape(rows // 32, 2, 16, channels)
    even, odd = tiles[:, 0], tiles[:, 1]
    own_ref[...] = jnp.where(core == 0, even, odd).reshape(rows // 2, channels).astype(BF16)
    other_ref[...] = jnp.where(core == 0, odd, even).reshape(rows // 2, channels).astype(BF16)


def state_mixer(
    mixer_in, doc_ids, lam_re, lam_im, log_step, log_keep, in_re, in_im, out_re, out_im, skip_gain
):
    rows, channels = mixer_in.shape
    groups, states = lam_re.shape
    width = groups * states
    previous = jnp.concatenate([doc_ids[:1], doc_ids[:-1]])
    keep = jnp.exp(log_keep) * (doc_ids == previous).astype(F32)[:, None]
    docs = (doc_ids[0] + 8 * doc_ids[-1]).astype(F32).reshape(1, 1)
    devices = lax.axis_size(SP)
    big = jax.ShapeDtypeStruct((width // LANES, rows, LANES), F32)
    send, finals, dre, dim, kx, a_rows = pl.pallas_call(
        drive_kernel,
        out_shape=(
            jax.ShapeDtypeStruct((devices, 4, width), F32),
            jax.ShapeDtypeStruct((3, CHUNKS, width), F32),
            big, big, big,
            jax.ShapeDtypeStruct((2, width), F32),
        ),
        name="drive",
    )(
        mixer_in, keep, docs, lam_re, lam_im, log_step.reshape(groups, 1),
        in_re.reshape(width, -1), in_im.reshape(width, -1),
    )
    got = lax.all_to_all(send, SP, 0, 0, tiled=True)
    place = jnp.stack([lax.axis_index(SP), lax.axis_index("core")]).astype(jnp.int32)
    half = jax.ShapeDtypeStruct((rows // 2, channels), BF16)
    in_vmem = pl.BlockSpec(memory_space=pltpu.VMEM)
    return pl.pallas_call(
        readout_kernel,
        out_shape=(half, half),
        in_specs=[pl.BlockSpec(memory_space=pltpu.SMEM)] + [in_vmem] * 10,
        scratch_shapes=[pltpu.VMEM(big.shape, F32), pltpu.VMEM(big.shape, F32)],
        name="readout",
    )(
        place, got, finals, dre, dim, kx, a_rows, mixer_in,
        out_re.reshape(channels, states), out_im.reshape(channels, states),
        skip_gain.reshape(1, channels),
    )


def dot(a, b):
    return jnp.dot(a, b, preferred_element_type=F32)


def on_device(
    residual, mixer_in, doc_ids, lam_re, lam_im, log_step, log_keep, in_re, in_im, out_re, out_im,
    skip_gain, w_val, w_gate, norm_gain, route_ids, route_wts, exp_gate, exp_up, exp_down,
    shared_gate, shared_up, shared_down,
):
    tok_loc, model_width = residual.shape
    layers = lax.axis_size("z")
    owners = lax.axis_size(SP)
    core = lax.axis_index("core")
    top_k = route_ids.shape[1]
    swap = lambda x: lax.ppermute(x, "core", [(0, 1), (1, 0)])
    pair_val, pair_gate = swap(w_val), swap(w_gate)
    pair_eg, pair_eu, pair_ed = swap(exp_gate[0]), swap(exp_up[0]), swap(exp_down[0])

    act_own, act_other = state_mixer(
        mixer_in, doc_ids, lam_re, lam_im, log_step, log_keep, in_re, in_im, out_re, out_im,
        skip_gain,
    )
    act_pair = swap(act_other)
    value = (dot(act_own, w_val) + dot(act_pair, pair_val)).astype(BF16)
    gate = (dot(act_own, w_gate) + dot(act_pair, pair_gate)).astype(BF16)
    parts = jnp.concatenate([value, gate], axis=1).reshape(layers, tok_loc, 2 * model_width)
    parts = lax.all_to_all(parts, "z", 0, 0, tiled=True)
    projected = jnp.sum(parts.astype(F32), axis=0)
    hidden = residual.astype(F32) + projected[:, :model_width] * jax.nn.sigmoid(
        projected[:, model_width:]
    )
    normed = (
        hidden * lax.rsqrt(jnp.mean(hidden * hidden, axis=-1, keepdims=True) + EPSILON) * norm_gain
    ).astype(BF16)

    tokens = layers * tok_loc
    mine = lambda x: lax.dynamic_index_in_dim(
        x.reshape(layers, 2, tok_loc, top_k), core, 1, keepdims=False
    )
    ids = mine(route_ids).reshape(layers, tok_loc * top_k)
    wts = mine(route_wts).reshape(tokens, top_k)
    same = ids[:, :, None] == ids[:, None, :]
    order = jnp.arange(tok_loc * top_k)
    rank = jnp.sum((same & (order[None, :] < order[:, None])).astype(jnp.int32), axis=-1)
    capacity = tok_loc * top_k // owners
    block = layers * capacity
    slots = ids * block + capacity * jnp.arange(layers, dtype=jnp.int32)[:, None] + rank
    slots = slots.reshape(tokens, top_k)
    hit = slots[:, :, None] == jnp.arange(owners * block, dtype=jnp.int32)[None, None, :]
    picker = jnp.sum(hit.astype(F32), axis=1).astype(BF16)
    weights_high, weights_low = halves(jnp.sum(jnp.where(hit, wts[:, :, None], 0.0), axis=1))

    every = jnp.broadcast_to(normed[None], (layers, tok_loc, model_width))
    every = lax.all_to_all(every, "z", 0, 0, tiled=True).reshape(tokens, model_width)
    shared_inner = (jax.nn.silu(dot(normed, shared_gate)) * dot(normed, shared_up)).astype(BF16)
    base = hidden + dot(shared_inner, shared_down)
    packed = lax.dot_general(
        picker, every, (((0,), (0,)), ((), ())), preferred_element_type=F32
    ).astype(BF16)
    rows = lax.all_to_all(packed.reshape(owners, block, model_width), SP, 0, 0, tiled=True)
    rows = rows.reshape(owners * block, model_width)
    inner_own = (jax.nn.silu(dot(rows, exp_gate[0])) * dot(rows, exp_up[0])).astype(BF16)
    inner_pair = (jax.nn.silu(dot(rows, pair_eg)) * dot(rows, pair_eu)).astype(BF16)
    partial = (dot(inner_own, exp_down[0]) + dot(inner_pair, pair_ed)).astype(BF16)
    back = lax.all_to_all(partial.reshape(owners, block, model_width), SP, 0, 0, tiled=True)
    back = back.reshape(owners * block, model_width)
    routed = (dot(weights_high, back) + dot(weights_low, back)).astype(BF16)
    routed = lax.all_to_all(routed.reshape(layers, tok_loc, model_width), "z", 0, 0, tiled=True)
    return (base + jnp.sum(routed.astype(F32), axis=0)).astype(BF16)


def solution(mesh):
    grid = Mesh(mesh.devices.reshape(4, 4, 8, 2), ("y", "x", "z", "core"))
    return jax.shard_map(
        on_device,
        mesh=grid,
        in_specs=(
            P(SP + TP, None),
            P(SP, TP),
            P(SP),
            P(TP, None),
            P(TP, None),
            P(TP),
            P(SP, TP),
            P(TP, None, None),
            P(TP, None, None),
            P(TP, None, None),
            P(TP, None, None),
            P(TP),
            P(TP, None),
            P(TP, None),
            P(),
            P(SP, None),
            P(SP, None),
            P(SP, None, TP),
            P(SP, None, TP),
            P(SP, TP, None),
            P(),
            P(),
            P(),
        ),
        out_specs=P(SP + TP, None),
        check_vma=False,
    )
```

```python
import jax
import jax.numpy as jnp
from jax import lax
from jax.experimental import pallas as pl
from jax.experimental.pallas import tpu as pltpu
from jax.sharding import Mesh, PartitionSpec as P

EPSILON = 1e-06
SP = ("y", "x")
TP = ("z", "core")
STEPS = 32
CHUNKS = 8
LANES = 128
F32 = jnp.float32
BF16 = jnp.bfloat16


def halves(x):
    high = x.astype(BF16)
    return high, (x - high.astype(F32)).astype(BF16)


def dot(a, b):
    return jnp.dot(a, b, preferred_element_type=F32)


def dot_nt(a, b):
    return lax.dot_general(a, b, (((1,), (1,)), ((), ())), preferred_element_type=F32)


def block_rows(parts, group_states):
    groups, states = parts.shape
    tiled = jnp.concatenate([parts] * groups, axis=1)
    lane_group = lax.broadcasted_iota(jnp.int32, tiled.shape, 1) // states
    row = lax.broadcasted_iota(jnp.int32, tiled.shape, 0)
    return jnp.sum(jnp.where(lane_group == row, tiled, 0.0), axis=0, keepdims=True)


def decay_rows(lam_re, lam_im, log_step):
    time_step = jnp.exp(log_step)
    magnitude = jnp.exp(lam_re * time_step)
    angle = lam_im * time_step
    return magnitude * jnp.cos(angle), magnitude * jnp.sin(angle)


def squared(re, im, times):
    for _ in range(times):
        re, im = re * re - im * im, 2.0 * re * im
    return re, im


def store_lanes(ref, x):
    for i in range(ref.shape[0]):
        ref[i] = x[:, i * LANES : (i + 1) * LANES]


def strided(ref, j):
    at = pl.ds(j, CHUNKS, stride=STEPS)
    return jnp.concatenate([ref[i, at, :] for i in range(ref.shape[0])], axis=1)


def group_masked(parts, groups):
    tiled = jnp.concatenate([parts] * groups, axis=1)
    row_group = lax.broadcasted_iota(jnp.int32, tiled.shape, 0) // (parts.shape[0] // groups)
    lane_group = lax.broadcasted_iota(jnp.int32, tiled.shape, 1) // parts.shape[1]
    return jnp.where(row_group == lane_group, tiled, 0.0)


def drive_kernel(
    u_ref, keep_ref, docs_ref, lam_re_ref, lam_im_ref, step_ref, in_re_ref, in_im_ref,
    send_ref, finals_ref, dre_ref, dim_ref, kx_ref, a_ref,
):
    lam_re, lam_im = lam_re_ref[...], lam_im_ref[...]
    groups, states = lam_re.shape
    width = groups * states
    square = (groups, groups)
    diagonal = lax.broadcasted_iota(jnp.int32, square, 0) == lax.broadcasted_iota(
        jnp.int32, square, 1
    )
    steps = jnp.broadcast_to(step_ref[...], square)
    log_step = jnp.sum(jnp.where(diagonal, steps, 0.0), axis=1, keepdims=True)
    dec_re, dec_im = decay_rows(lam_re, lam_im, log_step)
    denom = lam_re * lam_re + lam_im * lam_im
    less = dec_re - 1.0
    quot_re = block_rows((less * lam_re + dec_im * lam_im) / denom, states)
    quot_im = block_rows((dec_im * lam_re - less * lam_im) / denom, states)
    a_re, a_im = block_rows(dec_re, states), block_rows(dec_im, states)
    a_ref[0:1, :], a_ref[1:2, :] = a_re, a_im
    u = u_ref[...]

    def spread(ref):
        high, low = halves(group_masked(ref[...], groups))
        return dot(u, high) + dot(u, low)

    raw_re, raw_im = spread(in_re_ref), spread(in_im_ref)
    store_lanes(dre_ref, quot_re * raw_re - quot_im * raw_im)
    store_lanes(dim_ref, quot_re * raw_im + quot_im * raw_re)
    docs = docs_ref[...].astype(F32)
    previous = jnp.concatenate([docs[:, :1], docs[:, :-1]], axis=1)
    keep = jnp.exp(keep_ref[...]) * (docs == previous).astype(F32)
    high = keep.astype(BF16)
    rest = keep - high.astype(F32)
    middle = rest.astype(BF16)
    low = (rest - middle.astype(F32)).astype(BF16)
    split = jnp.concatenate(
        [high.astype(F32), middle.astype(F32), low.astype(F32), jnp.zeros_like(keep)], axis=0
    ).astype(BF16)
    expand = (
        lax.broadcasted_iota(jnp.int32, (4 * groups, width), 1) // states
        == lax.broadcasted_iota(jnp.int32, (4 * groups, width), 0) % groups
    ).astype(BF16)
    store_lanes(
        kx_ref,
        lax.dot_general(split, expand, (((0,), (0,)), ((), ())), preferred_element_type=F32),
    )
    wide = (CHUNKS, width)
    ar, ai = jnp.broadcast_to(a_re, wide), jnp.broadcast_to(a_im, wide)
    s_re, s_im = jnp.zeros(wide, F32), jnp.zeros(wide, F32)
    total = jnp.ones(wide, F32)
    for j in range(STEPS):
        k = strided(kx_ref, j)
        s_re, s_im = (
            k * (ar * s_re - ai * s_im) + strided(dre_ref, j),
            k * (ar * s_im + ai * s_re) + strided(dim_ref, j),
        )
        total = total * k
    finals_ref[0], finals_ref[1], finals_ref[2] = s_re, s_im, total
    b_re, b_im = squared(a_re, a_im, 5)
    c_re, c_im, kept = s_re[0:1], s_im[0:1], total[0:1]
    for c in range(1, CHUNKS):
        k = total[c : c + 1]
        c_re, c_im = (
            k * (b_re * c_re - b_im * c_im) + s_re[c : c + 1],
            k * (b_re * c_im + b_im * c_re) + s_im[c : c + 1],
        )
        kept = kept * k
    both = docs[:, :1] + 8.0 * docs[:, -1:]
    packed = jnp.concatenate([c_re, c_im, kept, jnp.broadcast_to(both, (1, width))], axis=0)
    send_ref[...] = jnp.broadcast_to(packed[None], send_ref.shape)


def readout_kernel(
    got_ref, finals_ref, dre_ref, dim_ref, kx_ref, a_ref, u_ref, out_re_ref, out_im_ref,
    skip_ref, own_ref, other_ref, sre_ref, sim_ref,
):
    position = lax.axis_index(SP)
    core = lax.axis_index("core")
    devices = got_ref.shape[0]
    width = a_ref.shape[1]
    a_re, a_im = a_ref[0:1, :], a_ref[1:2, :]
    b_re, b_im = squared(a_re, a_im, 5)
    w_re, w_im = squared(b_re, b_im, 3)
    c_re, c_im = jnp.zeros((1, width), F32), jnp.zeros((1, width), F32)
    closing = jnp.full((1, width), -1.0, F32)
    for i in range(devices):
        docs = got_ref[i, 3:4, :]
        last = jnp.floor(docs * 0.125)
        first = docs - 8.0 * last
        before = jnp.int32(i) < position
        here = jnp.int32(i) <= position
        linked = jnp.where(first == closing, 1.0, 0.0)
        c_re = jnp.where(here, linked * c_re, c_re)
        c_im = jnp.where(here, linked * c_im, c_im)
        k = got_ref[i, 2:3, :]
        n_re = k * (w_re * c_re - w_im * c_im) + got_ref[i, 0:1, :]
        n_im = k * (w_re * c_im + w_im * c_re) + got_ref[i, 1:2, :]
        c_re, c_im = jnp.where(before, n_re, c_re), jnp.where(before, n_im, c_im)
        closing = last
    heads_re, heads_im = [c_re], [c_im]
    for c in range(CHUNKS - 1):
        k = finals_ref[2, c : c + 1, :]
        c_re, c_im = (
            k * (b_re * c_re - b_im * c_im) + finals_ref[0, c : c + 1, :],
            k * (b_re * c_im + b_im * c_re) + finals_ref[1, c : c + 1, :],
        )
        heads_re.append(c_re)
        heads_im.append(c_im)
    s_re, s_im = jnp.concatenate(heads_re, axis=0), jnp.concatenate(heads_im, axis=0)
    wide = (CHUNKS, width)
    ar, ai = jnp.broadcast_to(a_re, wide), jnp.broadcast_to(a_im, wide)
    for j in range(STEPS):
        k = strided(kx_ref, j)
        s_re, s_im = (
            k * (ar * s_re - ai * s_im) + strided(dre_ref, j),
            k * (ar * s_im + ai * s_re) + strided(dim_ref, j),
        )
        for i in range(width // LANES):
            at = pl.ds(j, CHUNKS, stride=STEPS)
            sre_ref[i, at, :] = s_re[:, i * LANES : (i + 1) * LANES]
            sim_ref[i, at, :] = s_im[:, i * LANES : (i + 1) * LANES]
    rows, channels = u_ref.shape
    states = out_re_ref.shape[1]
    groups = width // states

    def gathered(state_ref, ref):
        high, low = halves(group_masked(ref[...], groups))
        blocks = [state_ref[i] for i in range(width // LANES)]
        s_high, s_low = halves(jnp.concatenate(blocks, axis=1))
        return dot_nt(s_high, high) + dot_nt(s_high, low) + dot_nt(s_low, high)

    readout = gathered(sre_ref, out_re_ref) - gathered(sim_ref, out_im_ref)
    readout = readout + skip_ref[...] * u_ref[...].astype(F32)
    active = jax.nn.gelu(readout)
    tiles = active.reshape(rows // 32, 2, 16, channels)
    even, odd = tiles[:, 0], tiles[:, 1]
    own_ref[...] = jnp.where(core == 0, even, odd).reshape(rows // 2, channels).astype(BF16)
    other_ref[...] = jnp.where(core == 0, odd, even).reshape(rows // 2, channels).astype(BF16)


def state_mixer(
    mixer_in, doc_ids, lam_re, lam_im, log_step, log_keep, in_re, in_im, out_re, out_im, skip_gain
):
    rows, channels = mixer_in.shape
    groups, states = lam_re.shape
    width = groups * states
    devices = lax.axis_size(SP)
    big = jax.ShapeDtypeStruct((width // LANES, rows, LANES), F32)
    send, finals, dre, dim, kx, a_rows = pl.pallas_call(
        drive_kernel,
        out_shape=(
            jax.ShapeDtypeStruct((devices, 4, width), F32),
            jax.ShapeDtypeStruct((3, CHUNKS, width), F32),
            big, big, big,
            jax.ShapeDtypeStruct((2, width), F32),
        ),
        name="drive",
    )(
        mixer_in, log_keep.T, doc_ids.reshape(1, rows), lam_re, lam_im,
        log_step.reshape(1, groups), jnp.swapaxes(in_re, 1, 2).reshape(channels, states),
        jnp.swapaxes(in_im, 1, 2).reshape(channels, states),
    )
    got = lax.all_to_all(send, SP, 0, 0, tiled=True)
    half = jax.ShapeDtypeStruct((rows // 2, channels), BF16)
    return pl.pallas_call(
        readout_kernel,
        out_shape=(half, half),
        scratch_shapes=[pltpu.VMEM(big.shape, F32), pltpu.VMEM(big.shape, F32)],
        name="readout",
    )(
        got, finals, dre, dim, kx, a_rows, mixer_in,
        out_re.reshape(channels, states), out_im.reshape(channels, states),
        skip_gain.reshape(1, channels),
    )


def gated_kernel(own_ref, pair_ref, wv_ref, wg_ref, pv_ref, pg_ref, out_ref):
    own, pair = own_ref[...], pair_ref[...]
    width = wv_ref.shape[1]
    layers, tok_loc, _ = out_ref.shape
    value = dot(own, wv_ref[...]) + dot(pair, pv_ref[...])
    out_ref[:, :, :width] = value.reshape(layers, tok_loc, width).astype(BF16)
    gate = dot(own, wg_ref[...]) + dot(pair, pg_ref[...])
    out_ref[:, :, width:] = gate.reshape(layers, tok_loc, width).astype(BF16)


def expert_kernel(rows_ref, g_ref, u_ref, d_ref, pg_ref, pu_ref, pd_ref, out_ref):
    rows = rows_ref[...]
    inner = (jax.nn.silu(dot(rows, g_ref[...])) * dot(rows, u_ref[...])).astype(BF16)
    pair = (jax.nn.silu(dot(rows, pg_ref[...])) * dot(rows, pu_ref[...])).astype(BF16)
    out_ref[...] = (dot(inner, d_ref[...]) + dot(pair, pd_ref[...])).astype(BF16)


def on_device(
    residual, mixer_in, doc_ids, lam_re, lam_im, log_step, log_keep, in_re, in_im, out_re, out_im,
    skip_gain, w_val, w_gate, norm_gain, route_ids, route_wts, exp_gate, exp_up, exp_down,
    shared_gate, shared_up, shared_down,
):
    tok_loc, model_width = residual.shape
    layers = lax.axis_size("z")
    owners = lax.axis_size(SP)
    core = lax.axis_index("core")
    top_k = route_ids.shape[1]
    swap = lambda x: lax.ppermute(x, "core", [(0, 1), (1, 0)])
    pair_val, pair_gate = swap(w_val), swap(w_gate)
    pair_eg, pair_eu, pair_ed = swap(exp_gate[0]), swap(exp_up[0]), swap(exp_down[0])

    act_own, act_other = state_mixer(
        mixer_in, doc_ids, lam_re, lam_im, log_step, log_keep, in_re, in_im, out_re, out_im,
        skip_gain,
    )
    act_pair = swap(act_other)
    parts = pl.pallas_call(
        gated_kernel,
        out_shape=jax.ShapeDtypeStruct((layers, tok_loc, 2 * model_width), BF16),
        name="gated",
    )(act_own, act_pair, w_val, w_gate, pair_val, pair_gate)
    parts = lax.all_to_all(parts, "z", 0, 0, tiled=True)
    projected = jnp.sum(parts.astype(F32), axis=0)
    hidden = residual.astype(F32) + projected[:, :model_width] * jax.nn.sigmoid(
        projected[:, model_width:]
    )
    normed = (
        hidden * lax.rsqrt(jnp.mean(hidden * hidden, axis=-1, keepdims=True) + EPSILON) * norm_gain
    ).astype(BF16)

    tokens = layers * tok_loc
    mine = lambda x: lax.dynamic_index_in_dim(
        x.reshape(layers, 2, tok_loc, top_k), core, 1, keepdims=False
    )
    ids = mine(route_ids).reshape(layers, tok_loc * top_k)
    wts = mine(route_wts).reshape(tokens, top_k)
    same = ids[:, :, None] == ids[:, None, :]
    order = jnp.arange(tok_loc * top_k)
    rank = jnp.sum((same & (order[None, :] < order[:, None])).astype(jnp.int32), axis=-1)
    capacity = tok_loc * top_k // owners
    block = layers * capacity
    slots = ids * block + capacity * jnp.arange(layers, dtype=jnp.int32)[:, None] + rank
    slots = slots.reshape(tokens, top_k)
    hit = slots[:, :, None] == jnp.arange(owners * block, dtype=jnp.int32)[None, None, :]
    picker = jnp.sum(hit.astype(F32), axis=1).astype(BF16)
    weights_high, weights_low = halves(jnp.sum(jnp.where(hit, wts[:, :, None], 0.0), axis=1))

    every = jnp.broadcast_to(normed[None], (layers, tok_loc, model_width))
    every = lax.all_to_all(every, "z", 0, 0, tiled=True).reshape(tokens, model_width)
    shared_inner = (jax.nn.silu(dot(normed, shared_gate)) * dot(normed, shared_up)).astype(BF16)
    base = hidden + dot(shared_inner, shared_down)
    every, base = lax.optimization_barrier((every, base))
    packed = lax.dot_general(
        picker, every, (((0,), (0,)), ((), ())), preferred_element_type=F32
    ).astype(BF16)
    rows = lax.all_to_all(packed.reshape(owners, block, model_width), SP, 0, 0, tiled=True)
    rows = rows.reshape(owners * block, model_width)
    partial = pl.pallas_call(
        expert_kernel, out_shape=jax.ShapeDtypeStruct(rows.shape, BF16), name="expert"
    )(rows, exp_gate[0], exp_up[0], exp_down[0], pair_eg, pair_eu, pair_ed)
    back = lax.all_to_all(partial.reshape(owners, block, model_width), SP, 0, 0, tiled=True)
    back = back.reshape(owners * block, model_width)
    routed = (dot(weights_high, back) + dot(weights_low, back)).astype(BF16)
    routed = lax.all_to_all(routed.reshape(layers, tok_loc, model_width), "z", 0, 0, tiled=True)
    return (base + jnp.sum(routed.astype(F32), axis=0)).astype(BF16)


def solution(mesh):
    grid = Mesh(mesh.devices.reshape(4, 4, 8, 2), ("y", "x", "z", "core"))
    return jax.shard_map(
        on_device,
        mesh=grid,
        in_specs=(
            P(SP + TP, None),
            P(SP, TP),
            P(SP),
            P(TP, None),
            P(TP, None),
            P(TP),
            P(SP, TP),
            P(TP, None, None),
            P(TP, None, None),
            P(TP, None, None),
            P(TP, None, None),
            P(TP),
            P(TP, None),
            P(TP, None),
            P(),
            P(SP, None),
            P(SP, None),
            P(SP, None, TP),
            P(SP, None, TP),
            P(SP, TP, None),
            P(),
            P(),
            P(),
        ),
        out_specs=P(SP + TP, None),
        check_vma=False,
    )
```

```python
import jax
import jax.numpy as jnp
from jax import lax
from jax.experimental import pallas as pl
from jax.experimental.pallas import tpu as pltpu
from jax.sharding import Mesh, PartitionSpec as P


EPSILON = 1e-06
SP = ("y", "x")
TP = ("zh", "zl", "core")
Z = ("zh", "zl")
STEPS = 32
CHUNKS = 8
LANES = 128
F32 = jnp.float32
BF16 = jnp.bfloat16


def halves(x):
    high = x.astype(BF16)
    return high, (x - high.astype(F32)).astype(BF16)


def dot(a, b):
    return jnp.dot(a, b, preferred_element_type=F32)


def dot_nt(a, b):
    return lax.dot_general(a, b, (((1,), (1,)), ((), ())), preferred_element_type=F32)


def block_rows(parts):
    groups, states = parts.shape
    tiled = jnp.concatenate([parts] * groups, axis=1)
    lane_group = lax.broadcasted_iota(jnp.int32, tiled.shape, 1) // states
    row = lax.broadcasted_iota(jnp.int32, tiled.shape, 0)
    return jnp.sum(jnp.where(lane_group == row, tiled, 0.0), axis=0, keepdims=True)


def decay_rows(lam_re, lam_im, log_step):
    time_step = jnp.exp(log_step)
    magnitude = jnp.exp(lam_re * time_step)
    angle = lam_im * time_step
    return magnitude * jnp.cos(angle), magnitude * jnp.sin(angle)


def squared(re, im, times):
    for _ in range(times):
        re, im = re * re - im * im, 2.0 * re * im
    return re, im


def store_lanes(ref, x):
    for i in range(ref.shape[0]):
        ref[i] = x[:, i * LANES : (i + 1) * LANES]


def strided(ref, j):
    at = pl.ds(j, CHUNKS, stride=STEPS)
    return jnp.concatenate([ref[i, at, :] for i in range(ref.shape[0])], axis=1)


def group_masked(parts, groups):
    tiled = jnp.concatenate([parts] * groups, axis=1)
    row_group = lax.broadcasted_iota(jnp.int32, tiled.shape, 0) // (parts.shape[0] // groups)
    lane_group = lax.broadcasted_iota(jnp.int32, tiled.shape, 1) // parts.shape[1]
    return jnp.where(row_group == lane_group, tiled, 0.0)


def drive_kernel(
    u_ref, keep_ref, docs_ref, lam_re_ref, lam_im_ref, step_ref, in_re_ref, in_im_ref,
    send_ref, finals_ref, dre_ref, dim_ref, kx_ref, a_ref,
):
    lam_re, lam_im = lam_re_ref[...], lam_im_ref[...]
    groups, states = lam_re.shape
    width = groups * states
    square = (groups, groups)
    diagonal = lax.broadcasted_iota(jnp.int32, square, 0) == lax.broadcasted_iota(
        jnp.int32, square, 1
    )
    steps = jnp.broadcast_to(step_ref[...], square)
    log_step = jnp.sum(jnp.where(diagonal, steps, 0.0), axis=1, keepdims=True)
    dec_re, dec_im = decay_rows(lam_re, lam_im, log_step)
    denom = lam_re * lam_re + lam_im * lam_im
    less = dec_re - 1.0
    quot_re = block_rows((less * lam_re + dec_im * lam_im) / denom)
    quot_im = block_rows((dec_im * lam_re - less * lam_im) / denom)
    a_re, a_im = block_rows(dec_re), block_rows(dec_im)
    a_ref[0:1, :], a_ref[1:2, :] = a_re, a_im
    u = u_ref[...]

    def spread(ref):
        high, low = halves(group_masked(ref[...], groups))
        return dot(u, high) + dot(u, low)

    raw_re, raw_im = spread(in_re_ref), spread(in_im_ref)
    store_lanes(dre_ref, quot_re * raw_re - quot_im * raw_im)
    store_lanes(dim_ref, quot_re * raw_im + quot_im * raw_re)
    docs = docs_ref[...].astype(F32)
    previous = jnp.concatenate([docs[:, :1], docs[:, :-1]], axis=1)
    keep = jnp.exp(keep_ref[...]) * (docs == previous).astype(F32)
    high = keep.astype(BF16)
    rest = keep - high.astype(F32)
    middle = rest.astype(BF16)
    low = (rest - middle.astype(F32)).astype(BF16)
    split = jnp.concatenate(
        [high.astype(F32), middle.astype(F32), low.astype(F32), jnp.zeros_like(keep)], axis=0
    ).astype(BF16)
    expand = (
        lax.broadcasted_iota(jnp.int32, (4 * groups, width), 1) // states
        == lax.broadcasted_iota(jnp.int32, (4 * groups, width), 0) % groups
    ).astype(BF16)
    store_lanes(
        kx_ref,
        lax.dot_general(split, expand, (((0,), (0,)), ((), ())), preferred_element_type=F32),
    )
    wide = (CHUNKS, width)
    ar, ai = jnp.broadcast_to(a_re, wide), jnp.broadcast_to(a_im, wide)
    s_re, s_im = jnp.zeros(wide, F32), jnp.zeros(wide, F32)
    total = jnp.ones(wide, F32)
    for j in range(STEPS):
        k = strided(kx_ref, j)
        s_re, s_im = (
            k * (ar * s_re - ai * s_im) + strided(dre_ref, j),
            k * (ar * s_im + ai * s_re) + strided(dim_ref, j),
        )
        total = total * k
    finals_ref[0], finals_ref[1], finals_ref[2] = s_re, s_im, total
    b_re, b_im = squared(a_re, a_im, 5)
    c_re, c_im, kept = s_re[0:1], s_im[0:1], total[0:1]
    for c in range(1, CHUNKS):
        k = total[c : c + 1]
        c_re, c_im = (
            k * (b_re * c_re - b_im * c_im) + s_re[c : c + 1],
            k * (b_re * c_im + b_im * c_re) + s_im[c : c + 1],
        )
        kept = kept * k
    both = docs[:, :1] + 8.0 * docs[:, -1:]
    packed = jnp.concatenate([c_re, c_im, kept, jnp.broadcast_to(both, (1, width))], axis=0)
    send_ref[...] = jnp.broadcast_to(packed[None], send_ref.shape)


def readout_kernel(
    got_ref, finals_ref, dre_ref, dim_ref, kx_ref, a_ref, u_ref, out_re_ref, out_im_ref,
    skip_ref, own_ref, other_ref, sre_ref, sim_ref,
):
    position = lax.axis_index(SP)
    side = lax.axis_index("zl")
    devices = got_ref.shape[0]
    width = a_ref.shape[1]
    a_re, a_im = a_ref[0:1, :], a_ref[1:2, :]
    b_re, b_im = squared(a_re, a_im, 5)
    w_re, w_im = squared(b_re, b_im, 3)
    c_re, c_im = jnp.zeros((1, width), F32), jnp.zeros((1, width), F32)
    closing = jnp.full((1, width), -1.0, F32)
    for i in range(devices):
        docs = got_ref[i, 3:4, :]
        last = jnp.floor(docs * 0.125)
        first = docs - 8.0 * last
        before = jnp.int32(i) < position
        here = jnp.int32(i) <= position
        linked = jnp.where(first == closing, 1.0, 0.0)
        c_re = jnp.where(here, linked * c_re, c_re)
        c_im = jnp.where(here, linked * c_im, c_im)
        k = got_ref[i, 2:3, :]
        n_re = k * (w_re * c_re - w_im * c_im) + got_ref[i, 0:1, :]
        n_im = k * (w_re * c_im + w_im * c_re) + got_ref[i, 1:2, :]
        c_re, c_im = jnp.where(before, n_re, c_re), jnp.where(before, n_im, c_im)
        closing = last
    heads_re, heads_im = [c_re], [c_im]
    for c in range(CHUNKS - 1):
        k = finals_ref[2, c : c + 1, :]
        c_re, c_im = (
            k * (b_re * c_re - b_im * c_im) + finals_ref[0, c : c + 1, :],
            k * (b_re * c_im + b_im * c_re) + finals_ref[1, c : c + 1, :],
        )
        heads_re.append(c_re)
        heads_im.append(c_im)
    s_re, s_im = jnp.concatenate(heads_re, axis=0), jnp.concatenate(heads_im, axis=0)
    wide = (CHUNKS, width)
    ar, ai = jnp.broadcast_to(a_re, wide), jnp.broadcast_to(a_im, wide)
    for j in range(STEPS):
        k = strided(kx_ref, j)
        s_re, s_im = (
            k * (ar * s_re - ai * s_im) + strided(dre_ref, j),
            k * (ar * s_im + ai * s_re) + strided(dim_ref, j),
        )
        for i in range(width // LANES):
            at = pl.ds(j, CHUNKS, stride=STEPS)
            sre_ref[i, at, :] = s_re[:, i * LANES : (i + 1) * LANES]
            sim_ref[i, at, :] = s_im[:, i * LANES : (i + 1) * LANES]
    rows, channels = u_ref.shape
    states = out_re_ref.shape[1]
    groups = width // states

    def gathered(state_ref, ref):
        high, low = halves(group_masked(ref[...], groups))
        blocks = [state_ref[i] for i in range(width // LANES)]
        s_high, s_low = halves(jnp.concatenate(blocks, axis=1))
        return dot_nt(s_high, high) + dot_nt(s_high, low) + dot_nt(s_low, high)

    readout = gathered(sre_ref, out_re_ref) - gathered(sim_ref, out_im_ref)
    readout = readout + skip_ref[...] * u_ref[...].astype(F32)
    active = jax.nn.gelu(readout)
    tiles = active.reshape(rows // 64, 2, 32, channels)
    even, odd = tiles[:, 0], tiles[:, 1]
    own_ref[...] = jnp.where(side == 0, even, odd).reshape(rows // 2, channels).astype(BF16)
    other_ref[...] = jnp.where(side == 0, odd, even).reshape(rows // 2, channels).astype(BF16)


def state_mixer(
    mixer_in, doc_ids, lam_re, lam_im, log_step, log_keep, in_re, in_im, out_re, out_im, skip_gain
):
    rows, channels = mixer_in.shape
    groups, states = lam_re.shape
    width = groups * states
    devices = lax.axis_size(SP)
    big = jax.ShapeDtypeStruct((width // LANES, rows, LANES), F32)
    send, finals, dre, dim, kx, a_rows = pl.pallas_call(
        drive_kernel,
        out_shape=(
            jax.ShapeDtypeStruct((devices, 4, width), F32),
            jax.ShapeDtypeStruct((3, CHUNKS, width), F32),
            big, big, big,
            jax.ShapeDtypeStruct((2, width), F32),
        ),
        name="drive",
    )(
        mixer_in, log_keep.T, doc_ids.reshape(1, rows), lam_re, lam_im,
        log_step.reshape(1, groups), jnp.swapaxes(in_re, 1, 2).reshape(channels, states),
        jnp.swapaxes(in_im, 1, 2).reshape(channels, states),
    )
    got = lax.all_to_all(send, SP, 0, 0, tiled=True)
    half = jax.ShapeDtypeStruct((rows // 2, channels), BF16)
    return pl.pallas_call(
        readout_kernel,
        out_shape=(half, half),
        scratch_shapes=[pltpu.VMEM(big.shape, F32), pltpu.VMEM(big.shape, F32)],
        name="readout",
    )(
        got, finals, dre, dim, kx, a_rows, mixer_in,
        out_re.reshape(channels, states), out_im.reshape(channels, states),
        skip_gain.reshape(1, channels),
    )


def gated_kernel(own_ref, pair_ref, wv_ref, wg_ref, fv_ref, fg_ref, keep_ref, send_ref):
    own, pair = own_ref[...], pair_ref[...]
    width = wv_ref.shape[1]
    near, tok_loc, _ = keep_ref.shape
    first = lax.axis_index("core") == 0
    for at, w_ref, f_ref in ((0, wv_ref, fv_ref), (width, wg_ref, fg_ref)):
        both = dot(own, w_ref[...]) + dot(pair, f_ref[...])
        both = both.reshape(near, 2, tok_loc, width)
        even, odd = both[:, 0], both[:, 1]
        keep_ref[:, :, at : at + width] = jnp.where(first, even, odd).astype(BF16)
        send_ref[:, :, at : at + width] = jnp.where(first, odd, even).astype(BF16)


def expert_kernel(rows_ref, g_ref, u_ref, d_ref, pg_ref, pu_ref, pd_ref, out_ref):
    rows = rows_ref[...]
    inner = (jax.nn.silu(dot(rows, g_ref[...])) * dot(rows, u_ref[...])).astype(BF16)
    pair = (jax.nn.silu(dot(rows, pg_ref[...])) * dot(rows, pu_ref[...])).astype(BF16)
    out_ref[...] = (dot(inner, d_ref[...]) + dot(pair, pd_ref[...])).astype(BF16)


def on_device(
    residual, mixer_in, doc_ids, lam_re, lam_im, log_step, log_keep, in_re, in_im, out_re, out_im,
    skip_gain, w_val, w_gate, norm_gain, route_ids, route_wts, exp_gate, exp_up, exp_down,
    shared_gate, shared_up, shared_down,
):
    tok_loc, model_width = residual.shape
    layers = lax.axis_size(Z)
    owners = lax.axis_size(SP)
    core = lax.axis_index("core")
    top_k = route_ids.shape[1]
    swap = lambda x: lax.ppermute(x, "core", [(0, 1), (1, 0)])
    cross = lambda x: lax.ppermute(x, "zl", [(0, 1), (1, 0)])
    near = lax.axis_size("zh")
    far_val, far_gate = cross(w_val), cross(w_gate)
    pair_eg, pair_eu, pair_ed = swap(exp_gate[0]), swap(exp_up[0]), swap(exp_down[0])

    act_own, act_other = state_mixer(
        mixer_in, doc_ids, lam_re, lam_im, log_step, log_keep, in_re, in_im, out_re, out_im,
        skip_gain,
    )
    act_pair = cross(act_other)
    kept, sent = pl.pallas_call(
        gated_kernel,
        out_shape=(
            jax.ShapeDtypeStruct((near, tok_loc, 2 * model_width), BF16),
            jax.ShapeDtypeStruct((near, tok_loc, 2 * model_width), BF16),
        ),
        name="gated",
    )(act_own, act_pair, w_val, w_gate, far_val, far_gate)
    parts = (kept.astype(F32) + swap(sent).astype(F32)).astype(BF16)
    parts = lax.all_to_all(parts, "zh", 0, 0, tiled=True)
    projected = jnp.sum(parts.astype(F32), axis=0)
    hidden = residual.astype(F32) + projected[:, :model_width] * jax.nn.sigmoid(
        projected[:, model_width:]
    )
    normed = (
        hidden * lax.rsqrt(jnp.mean(hidden * hidden, axis=-1, keepdims=True) + EPSILON) * norm_gain
    ).astype(BF16)

    tokens = layers * tok_loc
    mine = lambda x: lax.dynamic_index_in_dim(
        x.reshape(layers, 2, tok_loc, top_k), core, 1, keepdims=False
    )
    ids = mine(route_ids).reshape(layers, tok_loc * top_k)
    wts = mine(route_wts).reshape(tokens, top_k)
    same = ids[:, :, None] == ids[:, None, :]
    order = jnp.arange(tok_loc * top_k)
    rank = jnp.sum((same & (order[None, :] < order[:, None])).astype(jnp.int32), axis=-1)
    capacity = tok_loc * top_k // owners
    block = layers * capacity
    slots = ids * block + capacity * jnp.arange(layers, dtype=jnp.int32)[:, None] + rank
    slots = slots.reshape(tokens, top_k)
    hit = slots[:, :, None] == jnp.arange(owners * block, dtype=jnp.int32)[None, None, :]
    picker = jnp.sum(hit.astype(F32), axis=1).astype(BF16)
    weights_high, weights_low = halves(jnp.sum(jnp.where(hit, wts[:, :, None], 0.0), axis=1))

    every = jnp.broadcast_to(normed[None], (layers, tok_loc, model_width))
    every = lax.all_to_all(every, Z, 0, 0, tiled=True).reshape(tokens, model_width)
    shared_inner = (jax.nn.silu(dot(normed, shared_gate)) * dot(normed, shared_up)).astype(BF16)
    base = hidden + dot(shared_inner, shared_down)
    every, base = lax.optimization_barrier((every, base))
    packed = lax.dot_general(
        picker, every, (((0,), (0,)), ((), ())), preferred_element_type=F32
    ).astype(BF16)
    rows = lax.all_to_all(packed.reshape(owners, block, model_width), SP, 0, 0, tiled=True)
    rows = rows.reshape(owners * block, model_width)
    partial = pl.pallas_call(
        expert_kernel, out_shape=jax.ShapeDtypeStruct(rows.shape, BF16), name="expert"
    )(rows, exp_gate[0], exp_up[0], exp_down[0], pair_eg, pair_eu, pair_ed)
    back = lax.all_to_all(partial.reshape(owners, block, model_width), SP, 0, 0, tiled=True)
    back = back.reshape(owners * block, model_width)
    routed = (dot(weights_high, back) + dot(weights_low, back)).astype(BF16)
    routed = lax.all_to_all(routed.reshape(layers, tok_loc, model_width), Z, 0, 0, tiled=True)
    return (base + jnp.sum(routed.astype(F32), axis=0)).astype(BF16)


def solution(mesh):
    grid = Mesh(mesh.devices.reshape(4, 4, 4, 2, 2), ("y", "x", "zh", "zl", "core"))
    return jax.shard_map(
        on_device,
        mesh=grid,
        in_specs=(
            P(SP + TP, None),
            P(SP, TP),
            P(SP),
            P(TP, None),
            P(TP, None),
            P(TP),
            P(SP, TP),
            P(TP, None, None),
            P(TP, None, None),
            P(TP, None, None),
            P(TP, None, None),
            P(TP),
            P(TP, None),
            P(TP, None),
            P(),
            P(SP, None),
            P(SP, None),
            P(SP, None, TP),
            P(SP, None, TP),
            P(SP, TP, None),
            P(),
            P(),
            P(),
        ),
        out_specs=P(SP + TP, None),
        check_vma=False,
    )
```

```python
import jax
import jax.numpy as jnp
from jax import lax
from jax.experimental import pallas as pl
from jax.experimental.pallas import tpu as pltpu
from jax.sharding import Mesh, PartitionSpec as P


EPSILON = 1e-06
SP = ("y", "x")
TP = ("zh", "zl", "core")
Z = ("zh", "zl")
STEPS = 32
CHUNKS = 8
BLOCK = 64
SMALL = pltpu.CompilerParams(vmem_limit_bytes=16 * 2**20)
F32 = jnp.float32
BF16 = jnp.bfloat16


def halves(x):
    high = x.astype(BF16)
    return high, (x - high.astype(F32)).astype(BF16)


def in_hbm(x):
    return pltpu.with_memory_space_constraint(x, pltpu.HBM)


def call(kernel, outs, *operands):
    return pl.pallas_call(kernel, out_shape=outs, compiler_params=SMALL)(*operands)


def dot(a, b):
    return jnp.dot(a, b, preferred_element_type=F32)


def dot_nt(a, b):
    return lax.dot_general(a, b, (((1,), (1,)), ((), ())), preferred_element_type=F32)


def block_rows(parts):
    groups, states = parts.shape
    tiled = jnp.concatenate([parts] * groups, axis=1)
    lane_group = lax.broadcasted_iota(jnp.int32, tiled.shape, 1) // states
    row = lax.broadcasted_iota(jnp.int32, tiled.shape, 0)
    return jnp.sum(jnp.where(lane_group == row, tiled, 0.0), axis=0, keepdims=True)


def decay_rows(lam_re, lam_im, log_step):
    time_step = jnp.exp(log_step)
    magnitude = jnp.exp(lam_re * time_step)
    angle = lam_im * time_step
    return magnitude * jnp.cos(angle), magnitude * jnp.sin(angle)


def squared(re, im, times):
    for _ in range(times):
        re, im = re * re - im * im, 2.0 * re * im
    return re, im


def interleaved(rows):
    square = (rows, rows)
    row = lax.broadcasted_iota(jnp.int32, square, 0)
    source = (row % CHUNKS) * STEPS + row // CHUNKS
    found = lax.broadcasted_iota(jnp.int32, square, 1) == source
    return jnp.where(found, 1.0, 0.0).astype(BF16)


def tile(ref, j):
    return ref[j * CHUNKS : (j + 1) * CHUNKS, :]


def group_masked(parts, groups):
    tiled = jnp.concatenate([parts] * groups, axis=1)
    row_group = lax.broadcasted_iota(jnp.int32, tiled.shape, 0) // (parts.shape[0] // groups)
    lane_group = lax.broadcasted_iota(jnp.int32, tiled.shape, 1) // parts.shape[1]
    return jnp.where(row_group == lane_group, tiled, 0.0)


def fill_drive(
    u_ref, keep_ref, docs_ref, lam_re_ref, lam_im_ref, step_ref, in_re_ref, in_im_ref,
    dre_ref, dim_ref, kx_ref, mixed_ref, map_ref,
):
    lam_re, lam_im = lam_re_ref[...], lam_im_ref[...]
    groups, states = lam_re.shape
    width = groups * states
    square = (groups, groups)
    diagonal = lax.broadcasted_iota(jnp.int32, square, 0) == lax.broadcasted_iota(
        jnp.int32, square, 1
    )
    steps = jnp.broadcast_to(step_ref[...], square)
    log_step = jnp.sum(jnp.where(diagonal, steps, 0.0), axis=1, keepdims=True)
    dec_re, dec_im = decay_rows(lam_re, lam_im, log_step)
    denom = lam_re * lam_re + lam_im * lam_im
    less = dec_re - 1.0
    quot_re = block_rows((less * lam_re + dec_im * lam_im) / denom)
    quot_im = block_rows((dec_im * lam_re - less * lam_im) / denom)
    u = u_ref[...]
    for k, ref in enumerate((in_re_ref, in_im_ref)):
        map_ref[2 * k], map_ref[2 * k + 1] = halves(group_masked(ref[...], groups))
    order = interleaved(u.shape[0])
    mixed_ref[...] = dot(order, u).astype(BF16)
    docs = docs_ref[...].astype(F32)
    previous = jnp.concatenate([docs[:, :1], docs[:, :-1]], axis=1)
    keep = jnp.exp(keep_ref[...]) * (docs == previous).astype(F32)
    high = keep.astype(BF16)
    rest = keep - high.astype(F32)
    middle = rest.astype(BF16)
    low = (rest - middle.astype(F32)).astype(BF16)
    split = jnp.concatenate(
        [high.astype(F32), middle.astype(F32), low.astype(F32), jnp.zeros_like(keep)], axis=0
    ).astype(BF16)
    expand = (
        lax.broadcasted_iota(jnp.int32, (4 * groups, width), 1) // states
        == lax.broadcasted_iota(jnp.int32, (4 * groups, width), 0) % groups
    ).astype(BF16)
    split = dot_nt(split, order).astype(BF16)
    for start in range(0, u.shape[0], BLOCK):
        at = slice(start, start + BLOCK)
        part = mixed_ref[at, :]
        raw_re = dot(part, map_ref[0]) + dot(part, map_ref[1])
        raw_im = dot(part, map_ref[2]) + dot(part, map_ref[3])
        dre_ref[at, :] = quot_re * raw_re - quot_im * raw_im
        dim_ref[at, :] = quot_re * raw_im + quot_im * raw_re
        kx_ref[at, :] = lax.dot_general(
            split[:, at], expand, (((0,), (0,)), ((), ())), preferred_element_type=F32
        )
    return block_rows(dec_re), block_rows(dec_im), docs


def drive_kernel(*refs):
    inputs, (send_ref, finals_ref), scratch = refs[:8], refs[8:10], refs[10:]
    dre_ref, dim_ref, kx_ref = scratch[:3]
    a_re, a_im, docs = fill_drive(*inputs, *scratch)
    width = a_re.shape[1]
    wide = (CHUNKS, width)
    ar, ai = jnp.broadcast_to(a_re, wide), jnp.broadcast_to(a_im, wide)
    s_re, s_im = jnp.zeros(wide, F32), jnp.zeros(wide, F32)
    total = jnp.ones(wide, F32)
    for j in range(STEPS):
        k = tile(kx_ref, j)
        s_re, s_im = (
            k * (ar * s_re - ai * s_im) + tile(dre_ref, j),
            k * (ar * s_im + ai * s_re) + tile(dim_ref, j),
        )
        total = total * k
    finals_ref[0], finals_ref[1], finals_ref[2] = s_re, s_im, total
    b_re, b_im = squared(a_re, a_im, 5)
    c_re, c_im, kept = s_re[0:1], s_im[0:1], total[0:1]
    for c in range(1, CHUNKS):
        k = total[c : c + 1]
        c_re, c_im = (
            k * (b_re * c_re - b_im * c_im) + s_re[c : c + 1],
            k * (b_re * c_im + b_im * c_re) + s_im[c : c + 1],
        )
        kept = kept * k
    both = docs[:, :1] + 8.0 * docs[:, -1:]
    packed = jnp.concatenate([c_re, c_im, kept, jnp.broadcast_to(both, (1, width))], axis=0)
    send_ref[...] = jnp.broadcast_to(packed[None], send_ref.shape)


def readout_kernel(*refs):
    inputs, (got_ref, finals_ref, out_re_ref, out_im_ref, skip_ref) = refs[:8], refs[8:13]
    own_ref, other_ref, sre_ref, sim_ref, act_ref = refs[13:18]
    scratch = refs[18:]
    dre_ref, dim_ref, kx_ref, u_ref, map_ref = scratch
    a_re, a_im, _ = fill_drive(*inputs, *scratch)
    position = lax.axis_index(SP)
    side = lax.axis_index("zl")
    devices = got_ref.shape[0]
    width = a_re.shape[1]
    b_re, b_im = squared(a_re, a_im, 5)
    w_re, w_im = squared(b_re, b_im, 3)
    c_re, c_im = jnp.zeros((1, width), F32), jnp.zeros((1, width), F32)
    closing = jnp.full((1, width), -1.0, F32)
    for i in range(devices):
        docs = got_ref[i, 3:4, :]
        last = jnp.floor(docs * 0.125)
        first = docs - 8.0 * last
        before = jnp.int32(i) < position
        here = jnp.int32(i) <= position
        linked = jnp.where(first == closing, 1.0, 0.0)
        c_re = jnp.where(here, linked * c_re, c_re)
        c_im = jnp.where(here, linked * c_im, c_im)
        k = got_ref[i, 2:3, :]
        n_re = k * (w_re * c_re - w_im * c_im) + got_ref[i, 0:1, :]
        n_im = k * (w_re * c_im + w_im * c_re) + got_ref[i, 1:2, :]
        c_re, c_im = jnp.where(before, n_re, c_re), jnp.where(before, n_im, c_im)
        closing = last
    heads_re, heads_im = [c_re], [c_im]
    for c in range(CHUNKS - 1):
        k = finals_ref[2, c : c + 1, :]
        c_re, c_im = (
            k * (b_re * c_re - b_im * c_im) + finals_ref[0, c : c + 1, :],
            k * (b_re * c_im + b_im * c_re) + finals_ref[1, c : c + 1, :],
        )
        heads_re.append(c_re)
        heads_im.append(c_im)
    s_re, s_im = jnp.concatenate(heads_re, axis=0), jnp.concatenate(heads_im, axis=0)
    wide = (CHUNKS, width)
    ar, ai = jnp.broadcast_to(a_re, wide), jnp.broadcast_to(a_im, wide)
    for j in range(STEPS):
        k = tile(kx_ref, j)
        s_re, s_im = (
            k * (ar * s_re - ai * s_im) + tile(dre_ref, j),
            k * (ar * s_im + ai * s_re) + tile(dim_ref, j),
        )
        sre_ref[j * CHUNKS : (j + 1) * CHUNKS, :] = s_re
        sim_ref[j * CHUNKS : (j + 1) * CHUNKS, :] = s_im
    rows, channels = u_ref.shape
    states = out_re_ref.shape[1]
    groups = width // states

    for k, ref in enumerate((out_re_ref, out_im_ref)):
        map_ref[2 * k], map_ref[2 * k + 1] = halves(group_masked(ref[...], groups))

    def gathered(states, k):
        high, low = halves(states)
        return (
            dot_nt(high, map_ref[k]) + dot_nt(high, map_ref[k + 1]) + dot_nt(low, map_ref[k])
        )

    for start in range(0, rows, BLOCK):
        at = slice(start, start + BLOCK)
        readout = gathered(sre_ref[at, :], 0) - gathered(sim_ref[at, :], 2)
        readout = readout + skip_ref[...] * u_ref[at, :].astype(F32)
        act_ref[at, :] = jax.nn.gelu(readout).astype(BF16)
    active = lax.dot_general(
        interleaved(rows), act_ref[...], (((0,), (0,)), ((), ())), preferred_element_type=F32
    )
    tiles = active.reshape(rows // 64, 2, 32, channels)
    even, odd = tiles[:, 0], tiles[:, 1]
    own_ref[...] = jnp.where(side == 0, even, odd).reshape(rows // 2, channels).astype(BF16)
    other_ref[...] = jnp.where(side == 0, odd, even).reshape(rows // 2, channels).astype(BF16)


def state_mixer(
    mixer_in, doc_ids, lam_re, lam_im, log_step, log_keep, in_re, in_im, out_re, out_im, skip_gain
):
    rows, channels = mixer_in.shape
    groups, states = lam_re.shape
    width = groups * states
    devices = lax.axis_size(SP)
    inputs = (
        mixer_in, log_keep.T, doc_ids.reshape(1, rows), lam_re, lam_im,
        log_step.reshape(1, groups), jnp.swapaxes(in_re, 1, 2).reshape(channels, states),
        jnp.swapaxes(in_im, 1, 2).reshape(channels, states),
    )
    inputs = tuple(map(in_hbm, inputs))
    big = pltpu.VMEM((rows, width), F32)
    mixed = pltpu.VMEM((rows, channels), BF16)
    scratch = [big, big, big, mixed, pltpu.VMEM((4, channels, width), BF16)]
    send, finals = pl.pallas_call(
        drive_kernel,
        out_shape=(
            jax.ShapeDtypeStruct((devices, 4, width), F32),
            jax.ShapeDtypeStruct((3, CHUNKS, width), F32),
        ),
        scratch_shapes=scratch,
        name="drive",
        compiler_params=SMALL,
    )(*inputs)
    got = lax.all_to_all(send, SP, 0, 0, tiled=True)
    half = jax.ShapeDtypeStruct((rows // 2, channels), BF16)
    return pl.pallas_call(
        readout_kernel,
        out_shape=(half, half),
        scratch_shapes=[big, big, mixed, *scratch],
        name="readout",
        compiler_params=SMALL,
    )(
        *inputs, got, finals, in_hbm(out_re.reshape(channels, states)),
        in_hbm(out_im.reshape(channels, states)), in_hbm(skip_gain.reshape(1, channels)),
    )


def gated_kernel(own_ref, pair_ref, wv_ref, wg_ref, fv_ref, fg_ref, keep_ref, send_ref):
    own, pair = own_ref[...], pair_ref[...]
    width = wv_ref.shape[1]
    near, tok_loc, _ = keep_ref.shape
    first = lax.axis_index("core") == 0
    for at, w_ref, f_ref in ((0, wv_ref, fv_ref), (width, wg_ref, fg_ref)):
        both = dot(own, w_ref[...]) + dot(pair, f_ref[...])
        both = both.reshape(near, 2, tok_loc, width)
        even, odd = both[:, 0], both[:, 1]
        keep_ref[:, :, at : at + width] = jnp.where(first, even, odd).astype(BF16)
        send_ref[:, :, at : at + width] = jnp.where(first, odd, even).astype(BF16)


def sum_kernel(kept_ref, got_ref, out_ref):
    out_ref[...] = (kept_ref[...].astype(F32) + got_ref[...].astype(F32)).astype(BF16)


def norm_kernel(parts_ref, res_ref, gain_ref, every_ref, hidden_ref, normed_ref):
    width = res_ref.shape[1]
    value = jnp.sum(parts_ref[:, :, :width].astype(F32), axis=0)
    gate = jnp.sum(parts_ref[:, :, width:].astype(F32), axis=0)
    hidden = res_ref[...].astype(F32) + value * jax.nn.sigmoid(gate)
    mean = jnp.mean(hidden * hidden, axis=-1, keepdims=True)
    normed = (hidden * lax.rsqrt(mean + EPSILON) * gain_ref[...]).astype(BF16)
    hidden_ref[...] = hidden
    normed_ref[...] = normed
    every_ref[...] = jnp.broadcast_to(normed[None], every_ref.shape)


def expert_kernel(rows_ref, g_ref, u_ref, d_ref, pg_ref, pu_ref, pd_ref, out_ref):
    rows = rows_ref[...]
    inner = (jax.nn.silu(dot(rows, g_ref[...])) * dot(rows, u_ref[...])).astype(BF16)
    pair = (jax.nn.silu(dot(rows, pg_ref[...])) * dot(rows, pu_ref[...])).astype(BF16)
    out_ref[...] = (dot(inner, d_ref[...]) + dot(pair, pd_ref[...])).astype(BF16)


def on_device(
    residual, mixer_in, doc_ids, lam_re, lam_im, log_step, log_keep, in_re, in_im, out_re, out_im,
    skip_gain, w_val, w_gate, norm_gain, route_ids, route_wts, exp_gate, exp_up, exp_down,
    shared_gate, shared_up, shared_down,
):
    tok_loc, model_width = residual.shape
    layers = lax.axis_size(Z)
    owners = lax.axis_size(SP)
    core = lax.axis_index("core")
    top_k = route_ids.shape[1]
    swap = lambda x: lax.ppermute(x, "core", [(0, 1), (1, 0)])
    cross = lambda x: lax.ppermute(x, "zl", [(0, 1), (1, 0)])
    near = lax.axis_size("zh")
    far_val, far_gate = cross(w_val), cross(w_gate)
    gate_w, up_w, down_w = exp_gate[0], exp_up[0], exp_down[0]
    pair_eg, pair_eu, pair_ed = swap(gate_w), swap(up_w), swap(down_w)

    act_own, act_other = state_mixer(
        mixer_in, doc_ids, lam_re, lam_im, log_step, log_keep, in_re, in_im, out_re, out_im,
        skip_gain,
    )
    act_pair = cross(act_other)
    shape = jax.ShapeDtypeStruct((near, tok_loc, 2 * model_width), BF16)
    kept, sent = call(
        gated_kernel, (shape, shape),
        act_own, act_pair, in_hbm(w_val), in_hbm(w_gate), far_val, far_gate,
    )
    parts = call(sum_kernel, shape, kept, swap(sent))
    parts = lax.all_to_all(parts, "zh", 0, 0, tiled=True)
    every, hidden, normed = call(
        norm_kernel,
        (
            jax.ShapeDtypeStruct((layers, tok_loc, model_width), BF16),
            jax.ShapeDtypeStruct(residual.shape, F32),
            jax.ShapeDtypeStruct(residual.shape, BF16),
        ),
        parts, residual, norm_gain.reshape(1, model_width),
    )

    tokens = layers * tok_loc
    mine = lambda x: lax.dynamic_index_in_dim(
        x.reshape(layers, 2, tok_loc, top_k), core, 1, keepdims=False
    )
    ids = mine(route_ids).reshape(layers, tok_loc * top_k)
    wts = mine(route_wts).reshape(tokens, top_k)
    same = ids[:, :, None] == ids[:, None, :]
    order = jnp.arange(tok_loc * top_k)
    rank = jnp.sum((same & (order[None, :] < order[:, None])).astype(jnp.int32), axis=-1)
    capacity = tok_loc * top_k // owners
    block = layers * capacity
    slots = ids * block + capacity * jnp.arange(layers, dtype=jnp.int32)[:, None] + rank
    slots = slots.reshape(tokens, top_k)
    hit = slots[:, :, None] == jnp.arange(owners * block, dtype=jnp.int32)[None, None, :]
    picker = jnp.sum(hit.astype(F32), axis=1).astype(BF16)
    weights_high, weights_low = halves(jnp.sum(jnp.where(hit, wts[:, :, None], 0.0), axis=1))

    every = lax.all_to_all(every, Z, 0, 0, tiled=True).reshape(tokens, model_width)
    shared_inner = (jax.nn.silu(dot(normed, shared_gate)) * dot(normed, shared_up)).astype(BF16)
    base = hidden + dot(shared_inner, shared_down)
    every, base = lax.optimization_barrier((every, base))
    packed = lax.dot_general(
        picker, every, (((0,), (0,)), ((), ())), preferred_element_type=F32
    ).astype(BF16)
    rows = lax.all_to_all(packed.reshape(owners, block, model_width), SP, 0, 0, tiled=True)
    rows = rows.reshape(owners * block, model_width)
    operands = (rows, gate_w, up_w, down_w, pair_eg, pair_eu, pair_ed)
    partial = pl.pallas_call(
        expert_kernel,
        out_shape=jax.ShapeDtypeStruct(rows.shape, BF16),
        name="expert",
        compiler_params=SMALL,
    )(*operands)
    back = lax.all_to_all(partial.reshape(owners, block, model_width), SP, 0, 0, tiled=True)
    back = back.reshape(owners * block, model_width)
    routed = (dot(weights_high, back) + dot(weights_low, back)).astype(BF16)
    routed = lax.all_to_all(routed.reshape(layers, tok_loc, model_width), Z, 0, 0, tiled=True)
    return (base + jnp.sum(routed.astype(F32), axis=0)).astype(BF16)


def solution(mesh):
    grid = Mesh(mesh.devices.reshape(4, 4, 4, 2, 2), ("y", "x", "zh", "zl", "core"))
    return jax.shard_map(
        on_device,
        mesh=grid,
        in_specs=(
            P(SP + TP, None),
            P(SP, TP),
            P(SP),
            P(TP, None),
            P(TP, None),
            P(TP),
            P(SP, TP),
            P(TP, None, None),
            P(TP, None, None),
            P(TP, None, None),
            P(TP, None, None),
            P(TP),
            P(TP, None),
            P(TP, None),
            P(),
            P(SP, None),
            P(SP, None),
            P(SP, None, TP),
            P(SP, None, TP),
            P(SP, TP, None),
            P(),
            P(),
            P(),
        ),
        out_specs=P(SP + TP, None),
        check_vma=False,
    )
```

```python
import jax
import jax.numpy as jnp
from jax import lax
from jax.experimental import pallas as pl
from jax.experimental.pallas import tpu as pltpu
from jax.sharding import Mesh, PartitionSpec as P


EPSILON = 1e-06
SP = ("y", "x")
TP = ("zh", "zl", "core")
Z = ("zh", "zl")
STEPS = 32
CHUNKS = 8
BLOCK = 64
SMALL = pltpu.CompilerParams(vmem_limit_bytes=16 * 2**20)
F32 = jnp.float32
BF16 = jnp.bfloat16


def halves(x):
    high = x.astype(BF16)
    return high, (x - high.astype(F32)).astype(BF16)


def in_hbm(x):
    return pltpu.with_memory_space_constraint(x, pltpu.HBM)


def call(kernel, outs, *operands):
    return pl.pallas_call(kernel, out_shape=outs, compiler_params=SMALL)(*operands)


def dot(a, b):
    return jnp.dot(a, b, preferred_element_type=F32)


def dot_nt(a, b):
    return lax.dot_general(a, b, (((1,), (1,)), ((), ())), preferred_element_type=F32)


def block_rows(parts):
    groups, states = parts.shape
    tiled = jnp.concatenate([parts] * groups, axis=1)
    lane_group = lax.broadcasted_iota(jnp.int32, tiled.shape, 1) // states
    row = lax.broadcasted_iota(jnp.int32, tiled.shape, 0)
    return jnp.sum(jnp.where(lane_group == row, tiled, 0.0), axis=0, keepdims=True)


def decay_rows(lam_re, lam_im, log_step):
    time_step = jnp.exp(log_step)
    magnitude = jnp.exp(lam_re * time_step)
    angle = lam_im * time_step
    return magnitude * jnp.cos(angle), magnitude * jnp.sin(angle)


def squared(re, im, times):
    for _ in range(times):
        re, im = re * re - im * im, 2.0 * re * im
    return re, im


def interleaved(rows):
    square = (rows, rows)
    row = lax.broadcasted_iota(jnp.int32, square, 0)
    source = (row % CHUNKS) * STEPS + row // CHUNKS
    found = lax.broadcasted_iota(jnp.int32, square, 1) == source
    return jnp.where(found, 1.0, 0.0).astype(BF16)


def tile(ref, j):
    return ref[j * CHUNKS : (j + 1) * CHUNKS, :]


def group_masked(parts, groups):
    tiled = jnp.concatenate([parts] * groups, axis=1)
    row_group = lax.broadcasted_iota(jnp.int32, tiled.shape, 0) // (parts.shape[0] // groups)
    lane_group = lax.broadcasted_iota(jnp.int32, tiled.shape, 1) // parts.shape[1]
    return jnp.where(row_group == lane_group, tiled, 0.0)


def fill_drive(
    u_ref, keep_ref, docs_ref, lam_re_ref, lam_im_ref, step_ref, in_re_ref, in_im_ref,
    dre_ref, dim_ref, kx_ref, mixed_ref, map_ref,
):
    lam_re, lam_im = lam_re_ref[...], lam_im_ref[...]
    groups, states = lam_re.shape
    width = groups * states
    square = (groups, groups)
    diagonal = lax.broadcasted_iota(jnp.int32, square, 0) == lax.broadcasted_iota(
        jnp.int32, square, 1
    )
    steps = jnp.broadcast_to(step_ref[...], square)
    log_step = jnp.sum(jnp.where(diagonal, steps, 0.0), axis=1, keepdims=True)
    dec_re, dec_im = decay_rows(lam_re, lam_im, log_step)
    denom = lam_re * lam_re + lam_im * lam_im
    less = dec_re - 1.0
    quot_re = block_rows((less * lam_re + dec_im * lam_im) / denom)
    quot_im = block_rows((dec_im * lam_re - less * lam_im) / denom)
    u = u_ref[...]
    for k, ref in enumerate((in_re_ref, in_im_ref)):
        map_ref[2 * k], map_ref[2 * k + 1] = halves(group_masked(ref[...], groups))
    order = interleaved(u.shape[0])
    mixed_ref[...] = dot(order, u).astype(BF16)
    docs = docs_ref[...].astype(F32)
    previous = jnp.concatenate([docs[:, :1], docs[:, :-1]], axis=1)
    keep = jnp.exp(keep_ref[...]) * (docs == previous).astype(F32)
    high = keep.astype(BF16)
    rest = keep - high.astype(F32)
    middle = rest.astype(BF16)
    low = (rest - middle.astype(F32)).astype(BF16)
    split = jnp.concatenate(
        [high.astype(F32), middle.astype(F32), low.astype(F32), jnp.zeros_like(keep)], axis=0
    ).astype(BF16)
    expand = (
        lax.broadcasted_iota(jnp.int32, (4 * groups, width), 1) // states
        == lax.broadcasted_iota(jnp.int32, (4 * groups, width), 0) % groups
    ).astype(BF16)
    split = dot_nt(split, order).astype(BF16)
    for start in range(0, u.shape[0], BLOCK):
        at = slice(start, start + BLOCK)
        part = mixed_ref[at, :]
        raw_re = dot(part, map_ref[0]) + dot(part, map_ref[1])
        raw_im = dot(part, map_ref[2]) + dot(part, map_ref[3])
        dre_ref[at, :] = quot_re * raw_re - quot_im * raw_im
        dim_ref[at, :] = quot_re * raw_im + quot_im * raw_re
        kx_ref[at, :] = lax.dot_general(
            split[:, at], expand, (((0,), (0,)), ((), ())), preferred_element_type=F32
        )
    return block_rows(dec_re), block_rows(dec_im), docs


def drive_kernel(*refs):
    inputs, (send_ref, finals_ref), scratch = refs[:8], refs[8:10], refs[10:]
    dre_ref, dim_ref, kx_ref = scratch[:3]
    a_re, a_im, docs = fill_drive(*inputs, *scratch)
    width = a_re.shape[1]
    wide = (CHUNKS, width)
    ar, ai = jnp.broadcast_to(a_re, wide), jnp.broadcast_to(a_im, wide)
    s_re, s_im = jnp.zeros(wide, F32), jnp.zeros(wide, F32)
    total = jnp.ones(wide, F32)
    for j in range(STEPS):
        k = tile(kx_ref, j)
        s_re, s_im = (
            k * (ar * s_re - ai * s_im) + tile(dre_ref, j),
            k * (ar * s_im + ai * s_re) + tile(dim_ref, j),
        )
        total = total * k
    finals_ref[0], finals_ref[1], finals_ref[2] = s_re, s_im, total
    b_re, b_im = squared(a_re, a_im, 5)
    c_re, c_im, kept = s_re[0:1], s_im[0:1], total[0:1]
    for c in range(1, CHUNKS):
        k = total[c : c + 1]
        c_re, c_im = (
            k * (b_re * c_re - b_im * c_im) + s_re[c : c + 1],
            k * (b_re * c_im + b_im * c_re) + s_im[c : c + 1],
        )
        kept = kept * k
    both = docs[:, :1] + 8.0 * docs[:, -1:]
    packed = jnp.concatenate([c_re, c_im, kept, jnp.broadcast_to(both, (1, width))], axis=0)
    send_ref[...] = jnp.broadcast_to(packed[None], send_ref.shape)


def readout_kernel(*refs):
    inputs, (got_ref, finals_ref, out_re_ref, out_im_ref, skip_ref) = refs[:8], refs[8:13]
    own_ref, other_ref, sre_ref, sim_ref, act_ref = refs[13:18]
    scratch = refs[18:]
    dre_ref, dim_ref, kx_ref, u_ref, map_ref = scratch
    a_re, a_im, _ = fill_drive(*inputs, *scratch)
    position = lax.axis_index(SP)
    side = lax.axis_index("zl")
    devices = got_ref.shape[0]
    width = a_re.shape[1]
    b_re, b_im = squared(a_re, a_im, 5)
    w_re, w_im = squared(b_re, b_im, 3)
    c_re, c_im = jnp.zeros((1, width), F32), jnp.zeros((1, width), F32)
    closing = jnp.full((1, width), -1.0, F32)
    for i in range(devices):
        docs = got_ref[i, 3:4, :]
        last = jnp.floor(docs * 0.125)
        first = docs - 8.0 * last
        before = jnp.int32(i) < position
        here = jnp.int32(i) <= position
        linked = jnp.where(first == closing, 1.0, 0.0)
        c_re = jnp.where(here, linked * c_re, c_re)
        c_im = jnp.where(here, linked * c_im, c_im)
        k = got_ref[i, 2:3, :]
        n_re = k * (w_re * c_re - w_im * c_im) + got_ref[i, 0:1, :]
        n_im = k * (w_re * c_im + w_im * c_re) + got_ref[i, 1:2, :]
        c_re, c_im = jnp.where(before, n_re, c_re), jnp.where(before, n_im, c_im)
        closing = last
    heads_re, heads_im = [c_re], [c_im]
    for c in range(CHUNKS - 1):
        k = finals_ref[2, c : c + 1, :]
        c_re, c_im = (
            k * (b_re * c_re - b_im * c_im) + finals_ref[0, c : c + 1, :],
            k * (b_re * c_im + b_im * c_re) + finals_ref[1, c : c + 1, :],
        )
        heads_re.append(c_re)
        heads_im.append(c_im)
    s_re, s_im = jnp.concatenate(heads_re, axis=0), jnp.concatenate(heads_im, axis=0)
    wide = (CHUNKS, width)
    ar, ai = jnp.broadcast_to(a_re, wide), jnp.broadcast_to(a_im, wide)
    for j in range(STEPS):
        k = tile(kx_ref, j)
        s_re, s_im = (
            k * (ar * s_re - ai * s_im) + tile(dre_ref, j),
            k * (ar * s_im + ai * s_re) + tile(dim_ref, j),
        )
        sre_ref[j * CHUNKS : (j + 1) * CHUNKS, :] = s_re
        sim_ref[j * CHUNKS : (j + 1) * CHUNKS, :] = s_im
    rows, channels = u_ref.shape
    states = out_re_ref.shape[1]
    groups = width // states

    for k, ref in enumerate((out_re_ref, out_im_ref)):
        map_ref[2 * k], map_ref[2 * k + 1] = halves(group_masked(ref[...], groups))

    def gathered(states, k):
        high, low = halves(states)
        return (
            dot_nt(high, map_ref[k]) + dot_nt(high, map_ref[k + 1]) + dot_nt(low, map_ref[k])
        )

    for start in range(0, rows, BLOCK):
        at = slice(start, start + BLOCK)
        readout = gathered(sre_ref[at, :], 0) - gathered(sim_ref[at, :], 2)
        readout = readout + skip_ref[...] * u_ref[at, :].astype(F32)
        act_ref[at, :] = jax.nn.gelu(readout).astype(BF16)
    active = lax.dot_general(
        interleaved(rows), act_ref[...], (((0,), (0,)), ((), ())), preferred_element_type=F32
    )
    tiles = active.reshape(rows // 64, 2, 32, channels)
    even, odd = tiles[:, 0], tiles[:, 1]
    own_ref[...] = jnp.where(side == 0, even, odd).reshape(rows // 2, channels).astype(BF16)
    other_ref[...] = jnp.where(side == 0, odd, even).reshape(rows // 2, channels).astype(BF16)


def state_mixer(
    mixer_in, doc_ids, lam_re, lam_im, log_step, log_keep, in_re, in_im, out_re, out_im, skip_gain
):
    rows, channels = mixer_in.shape
    groups, states = lam_re.shape
    width = groups * states
    devices = lax.axis_size(SP)
    inputs = (
        mixer_in, log_keep.T, doc_ids.reshape(1, rows), lam_re, lam_im,
        log_step.reshape(1, groups), jnp.swapaxes(in_re, 1, 2).reshape(channels, states),
        jnp.swapaxes(in_im, 1, 2).reshape(channels, states),
    )
    inputs = tuple(map(in_hbm, inputs))
    big = pltpu.VMEM((rows, width), F32)
    mixed = pltpu.VMEM((rows, channels), BF16)
    scratch = [big, big, big, mixed, pltpu.VMEM((4, channels, width), BF16)]
    send, finals = pl.pallas_call(
        drive_kernel,
        out_shape=(
            jax.ShapeDtypeStruct((devices, 4, width), F32),
            jax.ShapeDtypeStruct((3, CHUNKS, width), F32),
        ),
        scratch_shapes=scratch,
        name="drive",
        compiler_params=SMALL,
    )(*inputs)
    got = lax.all_to_all(send, SP, 0, 0, tiled=True)
    half = jax.ShapeDtypeStruct((rows // 2, channels), BF16)
    return pl.pallas_call(
        readout_kernel,
        out_shape=(half, half),
        scratch_shapes=[big, big, mixed, *scratch],
        name="readout",
        compiler_params=SMALL,
    )(
        *inputs, got, finals, in_hbm(out_re.reshape(channels, states)),
        in_hbm(out_im.reshape(channels, states)), in_hbm(skip_gain.reshape(1, channels)),
    )


def gated_kernel(own_ref, pair_ref, wv_ref, wg_ref, fv_ref, fg_ref, keep_ref, send_ref):
    own, pair = own_ref[...], pair_ref[...]
    width = wv_ref.shape[1]
    near, tok_loc, _ = keep_ref.shape
    first = lax.axis_index("core") == 0
    for at, w_ref, f_ref in ((0, wv_ref, fv_ref), (width, wg_ref, fg_ref)):
        both = dot(own, w_ref[...]) + dot(pair, f_ref[...])
        both = both.reshape(near, 2, tok_loc, width)
        even, odd = both[:, 0], both[:, 1]
        keep_ref[:, :, at : at + width] = jnp.where(first, even, odd).astype(BF16)
        send_ref[:, :, at : at + width] = jnp.where(first, odd, even).astype(BF16)


def sum_kernel(kept_ref, got_ref, out_ref):
    out_ref[...] = (kept_ref[...].astype(F32) + got_ref[...].astype(F32)).astype(BF16)


def norm_kernel(parts_ref, res_ref, gain_ref, every_ref, hidden_ref, normed_ref):
    width = res_ref.shape[1]
    value = jnp.sum(parts_ref[:, :, :width].astype(F32), axis=0)
    gate = jnp.sum(parts_ref[:, :, width:].astype(F32), axis=0)
    hidden = res_ref[...].astype(F32) + value * jax.nn.sigmoid(gate)
    mean = jnp.mean(hidden * hidden, axis=-1, keepdims=True)
    normed = (hidden * lax.rsqrt(mean + EPSILON) * gain_ref[...]).astype(BF16)
    hidden_ref[...] = hidden
    normed_ref[...] = normed
    every_ref[...] = jnp.broadcast_to(normed[None], every_ref.shape)


def shared_kernel(normed_ref, hidden_ref, g_ref, u_ref, d_ref, out_ref):
    normed = normed_ref[...]
    inner = (jax.nn.silu(dot(normed, g_ref[...])) * dot(normed, u_ref[...])).astype(BF16)
    out_ref[...] = hidden_ref[...] + dot(inner, d_ref[...])


def inner_kernel(rows_ref, g_ref, u_ref, pg_ref, pu_ref, keep_ref, send_ref):
    rows = rows_ref[...]
    width = g_ref.shape[1]
    near = lax.axis_size("zh")
    count, block = rows.shape[0] // 2, 2 * near
    first = lax.axis_index("zl") == 0
    square = (rows.shape[0], rows.shape[0])
    out = lax.broadcasted_iota(jnp.int32, square, 0)
    turn = out // count
    source, rest = (out % count) // block, out % block
    side = jnp.where(first, turn, 1 - turn)
    place = source * 2 * block + (rest // 2) * 4 + side * 2 + rest % 2
    order = jnp.where(lax.broadcasted_iota(jnp.int32, square, 1) == place, 1.0, 0.0)
    order = order.astype(BF16)
    for k, (gate_ref, up_ref) in enumerate(((g_ref, u_ref), (pg_ref, pu_ref))):
        at = slice(k * width, (k + 1) * width)
        inner = jax.nn.silu(dot(rows, gate_ref[...])) * dot(rows, up_ref[...])
        moved = dot(order, inner.astype(BF16)).astype(BF16)
        keep_ref[:, at] = moved[:count]
        send_ref[:, at] = moved[count:]


def down_kernel(keep_ref, got_ref, d_ref, pd_ref, fd_ref, fpd_ref, out_ref):
    width = d_ref.shape[0]
    kept, got = keep_ref[...], got_ref[...]
    total = dot(kept[:, :width], d_ref[...]) + dot(kept[:, width:], pd_ref[...])
    total = total + dot(got[:, :width], fd_ref[...]) + dot(got[:, width:], fpd_ref[...])
    out_ref[...] = total.astype(BF16)


def on_device(
    residual, mixer_in, doc_ids, lam_re, lam_im, log_step, log_keep, in_re, in_im, out_re, out_im,
    skip_gain, w_val, w_gate, norm_gain, route_ids, route_wts, exp_gate, exp_up, exp_down,
    shared_gate, shared_up, shared_down,
):
    tok_loc, model_width = residual.shape
    layers = lax.axis_size(Z)
    owners = lax.axis_size(SP)
    top_k = route_ids.shape[1]
    swap = lambda x: lax.ppermute(x, "core", [(0, 1), (1, 0)])
    cross = lambda x: lax.ppermute(x, "zl", [(0, 1), (1, 0)])
    near = lax.axis_size("zh")
    far_val, far_gate = cross(w_val), cross(w_gate)
    gate_w, up_w, down_w = exp_gate[0], exp_up[0], exp_down[0]
    pair_eg, pair_eu, pair_ed = swap(gate_w), swap(up_w), swap(down_w)

    corner = 2 * lax.axis_index("zl") + lax.axis_index("core")
    act_own, act_other = state_mixer(
        mixer_in, doc_ids, lam_re, lam_im, log_step, log_keep, in_re, in_im, out_re, out_im,
        skip_gain,
    )
    act_pair = cross(act_other)
    shape = jax.ShapeDtypeStruct((near, tok_loc, 2 * model_width), BF16)
    kept, sent = call(
        gated_kernel, (shape, shape),
        act_own, act_pair, in_hbm(w_val), in_hbm(w_gate), far_val, far_gate,
    )
    parts = call(sum_kernel, shape, kept, swap(sent))
    parts = lax.all_to_all(parts, "zh", 0, 0, tiled=True)
    capacity = tok_loc * top_k // owners

    def placed(ids, wts, count):
        ids = ids.reshape(count, tok_loc * top_k)
        same = ids[:, :, None] == ids[:, None, :]
        order = jnp.arange(tok_loc * top_k)
        rank = jnp.sum((same & (order[None, :] < order[:, None])).astype(jnp.int32), axis=-1)
        block = count * capacity
        slots = ids * block + capacity * jnp.arange(count, dtype=jnp.int32)[:, None] + rank
        slots = slots.reshape(count * tok_loc, top_k)
        hit = slots[:, :, None] == jnp.arange(owners * block, dtype=jnp.int32)[None, None, :]
        if wts is None:
            return jnp.sum(hit.astype(F32), axis=1).astype(BF16)
        wts = wts.reshape(count * tok_loc, top_k)
        return halves(jnp.sum(jnp.where(hit, wts[:, :, None], 0.0), axis=1))

    def mine(x, count, parts, at):
        x = x.reshape(count, parts, tok_loc, top_k)
        return lax.dynamic_index_in_dim(x, at, 1, keepdims=False)

    block = layers * capacity
    picker = placed(mine(route_ids, layers, 2, lax.axis_index("core")), None, layers)
    weights_high, weights_low = placed(
        mine(route_ids, near, 4, corner), mine(route_wts, near, 4, corner), near
    )
    parts, picker, weights_high, weights_low = lax.optimization_barrier(
        (parts, picker, weights_high, weights_low)
    )
    every, hidden, normed = call(
        norm_kernel,
        (
            jax.ShapeDtypeStruct((layers, tok_loc, model_width), BF16),
            jax.ShapeDtypeStruct(residual.shape, F32),
            jax.ShapeDtypeStruct(residual.shape, BF16),
        ),
        parts, residual, norm_gain.reshape(1, model_width),
    )

    tokens = layers * tok_loc
    every = lax.all_to_all(every, Z, 0, 0, tiled=True).reshape(tokens, model_width)
    base = call(
        shared_kernel, jax.ShapeDtypeStruct(hidden.shape, F32),
        normed, hidden, *map(in_hbm, (shared_gate, shared_up, shared_down)),
    )
    every, base, down_now = lax.optimization_barrier((every, base, down_w))
    far_down = cross(down_now)
    far_pair = swap(far_down)
    packed = lax.dot_general(
        picker, every, (((0,), (0,)), ((), ())), preferred_element_type=F32
    ).astype(BF16)
    rows = lax.all_to_all(packed.reshape(owners, block, model_width), SP, 0, 0, tiled=True)
    rows = rows.reshape(owners * block, model_width)
    half = owners * block // 2
    narrow = jax.ShapeDtypeStruct((half, 2 * gate_w.shape[1]), BF16)
    kept, sent = call(
        inner_kernel, (narrow, narrow), rows, *map(in_hbm, (gate_w, up_w, pair_eg, pair_eu)),
    )
    partial = call(
        down_kernel,
        jax.ShapeDtypeStruct((half, model_width), BF16),
        kept, cross(sent), in_hbm(down_w), in_hbm(pair_ed), far_down, far_pair,
    )
    back = lax.all_to_all(
        partial.reshape(owners, block // 2, model_width), SP, 0, 0, tiled=True
    ).reshape(half, model_width)
    routed = (dot(weights_high, back) + dot(weights_low, back)).astype(BF16)
    routed = lax.all_to_all(routed.reshape(near, tok_loc, model_width), "zh", 0, 0, tiled=True)
    return (base + jnp.sum(routed.astype(F32), axis=0)).astype(BF16)


def solution(mesh):
    grid = Mesh(mesh.devices.reshape(4, 4, 4, 2, 2), ("y", "x", "zh", "zl", "core"))
    return jax.shard_map(
        on_device,
        mesh=grid,
        in_specs=(
            P(SP + TP, None),
            P(SP, TP),
            P(SP),
            P(TP, None),
            P(TP, None),
            P(TP),
            P(SP, TP),
            P(TP, None, None),
            P(TP, None, None),
            P(TP, None, None),
            P(TP, None, None),
            P(TP),
            P(TP, None),
            P(TP, None),
            P(),
            P(SP, None),
            P(SP, None),
            P(SP, None, TP),
            P(SP, None, TP),
            P(SP, TP, None),
            P(),
            P(),
            P(),
        ),
        out_specs=P(SP + TP, None),
        check_vma=False,
    )
```

```python
import jax
import jax.numpy as jnp
from jax import lax
from jax.experimental import pallas as pl
from jax.experimental.pallas import tpu as pltpu
from jax.sharding import Mesh, PartitionSpec as P


EPSILON = 1e-06
SP = ("y", "x")
TP = ("zh", "zl", "core")
Z = ("zh", "zl")
STEPS = 32
CHUNKS = 8
BLOCK = 64
SMALL = pltpu.CompilerParams(vmem_limit_bytes=16 * 2**20)
F32 = jnp.float32
BF16 = jnp.bfloat16


def halves(x):
    high = x.astype(BF16)
    return high, (x - high.astype(F32)).astype(BF16)


def in_hbm(x):
    return pltpu.with_memory_space_constraint(x, pltpu.HBM)


def call(kernel, outs, *operands):
    return pl.pallas_call(kernel, out_shape=outs, compiler_params=SMALL)(*operands)


def dot(a, b):
    return jnp.dot(a, b, preferred_element_type=F32)


def dot_nt(a, b):
    return lax.dot_general(a, b, (((1,), (1,)), ((), ())), preferred_element_type=F32)


def block_rows(parts):
    groups, states = parts.shape
    tiled = jnp.concatenate([parts] * groups, axis=1)
    lane_group = lax.broadcasted_iota(jnp.int32, tiled.shape, 1) // states
    row = lax.broadcasted_iota(jnp.int32, tiled.shape, 0)
    return jnp.sum(jnp.where(lane_group == row, tiled, 0.0), axis=0, keepdims=True)


def decay_rows(lam_re, lam_im, log_step):
    time_step = jnp.exp(log_step)
    magnitude = jnp.exp(lam_re * time_step)
    angle = lam_im * time_step
    return magnitude * jnp.cos(angle), magnitude * jnp.sin(angle)


def squared(re, im, times):
    for _ in range(times):
        re, im = re * re - im * im, 2.0 * re * im
    return re, im


def interleaved(rows):
    square = (rows, rows)
    row = lax.broadcasted_iota(jnp.int32, square, 0)
    source = (row % CHUNKS) * STEPS + row // CHUNKS
    found = lax.broadcasted_iota(jnp.int32, square, 1) == source
    return jnp.where(found, 1.0, 0.0).astype(BF16)


def tile(ref, j):
    return ref[j * CHUNKS : (j + 1) * CHUNKS, :]


def group_masked(parts, groups):
    tiled = jnp.concatenate([parts] * groups, axis=1)
    row_group = lax.broadcasted_iota(jnp.int32, tiled.shape, 0) // (parts.shape[0] // groups)
    lane_group = lax.broadcasted_iota(jnp.int32, tiled.shape, 1) // parts.shape[1]
    return jnp.where(row_group == lane_group, tiled, 0.0)


def fill_drive(
    u_ref, keep_ref, docs_ref, lam_re_ref, lam_im_ref, step_ref, in_re_ref, in_im_ref,
    dre_ref, dim_ref, kx_ref, mixed_ref, map_ref,
):
    lam_re, lam_im = lam_re_ref[...], lam_im_ref[...]
    groups, states = lam_re.shape
    width = groups * states
    square = (groups, groups)
    diagonal = lax.broadcasted_iota(jnp.int32, square, 0) == lax.broadcasted_iota(
        jnp.int32, square, 1
    )
    steps = jnp.broadcast_to(step_ref[...], square)
    log_step = jnp.sum(jnp.where(diagonal, steps, 0.0), axis=1, keepdims=True)
    dec_re, dec_im = decay_rows(lam_re, lam_im, log_step)
    denom = lam_re * lam_re + lam_im * lam_im
    less = dec_re - 1.0
    quot_re = block_rows((less * lam_re + dec_im * lam_im) / denom)
    quot_im = block_rows((dec_im * lam_re - less * lam_im) / denom)
    u = u_ref[...]
    for k, ref in enumerate((in_re_ref, in_im_ref)):
        map_ref[2 * k], map_ref[2 * k + 1] = halves(group_masked(ref[...], groups))
    order = interleaved(u.shape[0])
    mixed_ref[...] = dot(order, u).astype(BF16)
    docs = docs_ref[...].astype(F32)
    previous = jnp.concatenate([docs[:, :1], docs[:, :-1]], axis=1)
    keep = jnp.exp(keep_ref[...]) * (docs == previous).astype(F32)
    high = keep.astype(BF16)
    rest = keep - high.astype(F32)
    middle = rest.astype(BF16)
    low = (rest - middle.astype(F32)).astype(BF16)
    split = jnp.concatenate(
        [high.astype(F32), middle.astype(F32), low.astype(F32), jnp.zeros_like(keep)], axis=0
    ).astype(BF16)
    expand = (
        lax.broadcasted_iota(jnp.int32, (4 * groups, width), 1) // states
        == lax.broadcasted_iota(jnp.int32, (4 * groups, width), 0) % groups
    ).astype(BF16)
    split = dot_nt(split, order).astype(BF16)
    for start in range(0, u.shape[0], BLOCK):
        at = slice(start, start + BLOCK)
        part = mixed_ref[at, :]
        raw_re = dot(part, map_ref[0]) + dot(part, map_ref[1])
        raw_im = dot(part, map_ref[2]) + dot(part, map_ref[3])
        dre_ref[at, :] = quot_re * raw_re - quot_im * raw_im
        dim_ref[at, :] = quot_re * raw_im + quot_im * raw_re
        kx_ref[at, :] = lax.dot_general(
            split[:, at], expand, (((0,), (0,)), ((), ())), preferred_element_type=F32
        )
    return block_rows(dec_re), block_rows(dec_im), docs


def drive_kernel(*refs):
    inputs, (send_ref, finals_ref), scratch = refs[:8], refs[8:10], refs[10:]
    dre_ref, dim_ref, kx_ref = scratch[:3]
    a_re, a_im, docs = fill_drive(*inputs, *scratch)
    width = a_re.shape[1]
    wide = (CHUNKS, width)
    ar, ai = jnp.broadcast_to(a_re, wide), jnp.broadcast_to(a_im, wide)
    s_re, s_im = jnp.zeros(wide, F32), jnp.zeros(wide, F32)
    total = jnp.ones(wide, F32)
    for j in range(STEPS):
        k = tile(kx_ref, j)
        s_re, s_im = (
            k * (ar * s_re - ai * s_im) + tile(dre_ref, j),
            k * (ar * s_im + ai * s_re) + tile(dim_ref, j),
        )
        total = total * k
    finals_ref[0], finals_ref[1], finals_ref[2] = s_re, s_im, total
    b_re, b_im = squared(a_re, a_im, 5)
    c_re, c_im, kept = s_re[0:1], s_im[0:1], total[0:1]
    for c in range(1, CHUNKS):
        k = total[c : c + 1]
        c_re, c_im = (
            k * (b_re * c_re - b_im * c_im) + s_re[c : c + 1],
            k * (b_re * c_im + b_im * c_re) + s_im[c : c + 1],
        )
        kept = kept * k
    both = docs[:, :1] + 8.0 * docs[:, -1:]
    packed = jnp.concatenate([c_re, c_im, kept, jnp.broadcast_to(both, (1, width))], axis=0)
    send_ref[...] = jnp.broadcast_to(packed[None], send_ref.shape)


def readout_kernel(*refs):
    inputs, (got_ref, finals_ref, out_re_ref, out_im_ref, skip_ref) = refs[:8], refs[8:13]
    own_ref, other_ref, sre_ref, sim_ref, act_ref = refs[13:18]
    scratch = refs[18:]
    dre_ref, dim_ref, kx_ref, u_ref, map_ref = scratch
    a_re, a_im, _ = fill_drive(*inputs, *scratch)
    position = lax.axis_index(SP)
    side = lax.axis_index("zl")
    devices = got_ref.shape[0]
    width = a_re.shape[1]
    b_re, b_im = squared(a_re, a_im, 5)
    w_re, w_im = squared(b_re, b_im, 3)
    c_re, c_im = jnp.zeros((1, width), F32), jnp.zeros((1, width), F32)
    closing = jnp.full((1, width), -1.0, F32)
    for i in range(devices):
        docs = got_ref[i, 3:4, :]
        last = jnp.floor(docs * 0.125)
        first = docs - 8.0 * last
        before = jnp.int32(i) < position
        here = jnp.int32(i) <= position
        linked = jnp.where(first == closing, 1.0, 0.0)
        c_re = jnp.where(here, linked * c_re, c_re)
        c_im = jnp.where(here, linked * c_im, c_im)
        k = got_ref[i, 2:3, :]
        n_re = k * (w_re * c_re - w_im * c_im) + got_ref[i, 0:1, :]
        n_im = k * (w_re * c_im + w_im * c_re) + got_ref[i, 1:2, :]
        c_re, c_im = jnp.where(before, n_re, c_re), jnp.where(before, n_im, c_im)
        closing = last
    heads_re, heads_im = [c_re], [c_im]
    for c in range(CHUNKS - 1):
        k = finals_ref[2, c : c + 1, :]
        c_re, c_im = (
            k * (b_re * c_re - b_im * c_im) + finals_ref[0, c : c + 1, :],
            k * (b_re * c_im + b_im * c_re) + finals_ref[1, c : c + 1, :],
        )
        heads_re.append(c_re)
        heads_im.append(c_im)
    s_re, s_im = jnp.concatenate(heads_re, axis=0), jnp.concatenate(heads_im, axis=0)
    wide = (CHUNKS, width)
    ar, ai = jnp.broadcast_to(a_re, wide), jnp.broadcast_to(a_im, wide)
    for j in range(STEPS):
        k = tile(kx_ref, j)
        s_re, s_im = (
            k * (ar * s_re - ai * s_im) + tile(dre_ref, j),
            k * (ar * s_im + ai * s_re) + tile(dim_ref, j),
        )
        sre_ref[j * CHUNKS : (j + 1) * CHUNKS, :] = s_re
        sim_ref[j * CHUNKS : (j + 1) * CHUNKS, :] = s_im
    rows, channels = u_ref.shape
    states = out_re_ref.shape[1]
    groups = width // states

    for k, ref in enumerate((out_re_ref, out_im_ref)):
        map_ref[2 * k], map_ref[2 * k + 1] = halves(group_masked(ref[...], groups))

    def gathered(states, k):
        high, low = halves(states)
        return (
            dot_nt(high, map_ref[k]) + dot_nt(high, map_ref[k + 1]) + dot_nt(low, map_ref[k])
        )

    for start in range(0, rows, BLOCK):
        at = slice(start, start + BLOCK)
        readout = gathered(sre_ref[at, :], 0) - gathered(sim_ref[at, :], 2)
        readout = readout + skip_ref[...] * u_ref[at, :].astype(F32)
        act_ref[at, :] = jax.nn.gelu(readout).astype(BF16)
    active = lax.dot_general(
        interleaved(rows), act_ref[...], (((0,), (0,)), ((), ())), preferred_element_type=F32
    )
    tiles = active.reshape(rows // 64, 2, 32, channels)
    even, odd = tiles[:, 0], tiles[:, 1]
    own_ref[...] = jnp.where(side == 0, even, odd).reshape(rows // 2, channels).astype(BF16)
    other_ref[...] = jnp.where(side == 0, odd, even).reshape(rows // 2, channels).astype(BF16)


def state_mixer(
    mixer_in, doc_ids, lam_re, lam_im, log_step, log_keep, in_re, in_im, out_re, out_im, skip_gain
):
    rows, channels = mixer_in.shape
    groups, states = lam_re.shape
    width = groups * states
    devices = lax.axis_size(SP)
    inputs = (
        mixer_in, log_keep.T, doc_ids.reshape(1, rows), lam_re, lam_im,
        log_step.reshape(1, groups), jnp.swapaxes(in_re, 1, 2).reshape(channels, states),
        jnp.swapaxes(in_im, 1, 2).reshape(channels, states),
    )
    inputs = tuple(map(in_hbm, inputs))
    big = pltpu.VMEM((rows, width), F32)
    mixed = pltpu.VMEM((rows, channels), BF16)
    scratch = [big, big, big, mixed, pltpu.VMEM((4, channels, width), BF16)]
    send, finals = pl.pallas_call(
        drive_kernel,
        out_shape=(
            jax.ShapeDtypeStruct((devices, 4, width), F32),
            jax.ShapeDtypeStruct((3, CHUNKS, width), F32),
        ),
        scratch_shapes=scratch,
        name="drive",
        compiler_params=SMALL,
    )(*inputs)
    got = lax.all_to_all(send, SP, 0, 0, tiled=True)
    half = jax.ShapeDtypeStruct((rows // 2, channels), BF16)
    return pl.pallas_call(
        readout_kernel,
        out_shape=(half, half),
        scratch_shapes=[big, big, mixed, *scratch],
        name="readout",
        compiler_params=SMALL,
    )(
        *inputs, got, finals, in_hbm(out_re.reshape(channels, states)),
        in_hbm(out_im.reshape(channels, states)), in_hbm(skip_gain.reshape(1, channels)),
    )


def gated_kernel(own_ref, pair_ref, wv_ref, wg_ref, fv_ref, fg_ref, keep_ref, send_ref):
    own, pair = own_ref[...], pair_ref[...]
    width = wv_ref.shape[1]
    near, tok_loc, _ = keep_ref.shape
    first = lax.axis_index("core") == 0
    for at, w_ref, f_ref in ((0, wv_ref, fv_ref), (width, wg_ref, fg_ref)):
        both = dot(own, w_ref[...]) + dot(pair, f_ref[...])
        both = both.reshape(near, 2, tok_loc, width)
        even, odd = both[:, 0], both[:, 1]
        keep_ref[:, :, at : at + width] = jnp.where(first, even, odd).astype(BF16)
        send_ref[:, :, at : at + width] = jnp.where(first, odd, even).astype(BF16)


def sum_kernel(kept_ref, got_ref, out_ref):
    out_ref[...] = (kept_ref[...].astype(F32) + got_ref[...].astype(F32)).astype(BF16)


def norm_kernel(parts_ref, res_ref, gain_ref, every_ref, hidden_ref, normed_ref):
    width = res_ref.shape[1]
    value = jnp.sum(parts_ref[:, :, :width].astype(F32), axis=0)
    gate = jnp.sum(parts_ref[:, :, width:].astype(F32), axis=0)
    hidden = res_ref[...].astype(F32) + value * jax.nn.sigmoid(gate)
    mean = jnp.mean(hidden * hidden, axis=-1, keepdims=True)
    normed = (hidden * lax.rsqrt(mean + EPSILON) * gain_ref[...]).astype(BF16)
    hidden_ref[...] = hidden
    normed_ref[...] = normed
    every_ref[...] = jnp.broadcast_to(normed[None], every_ref.shape)


def shared_kernel(normed_ref, hidden_ref, g_ref, u_ref, d_ref, out_ref):
    normed = normed_ref[...]
    inner = (jax.nn.silu(dot(normed, g_ref[...])) * dot(normed, u_ref[...])).astype(BF16)
    out_ref[...] = hidden_ref[...] + dot(inner, d_ref[...])


def side_rows(rows, kept):
    near = lax.axis_size("zh")
    count, block = rows.shape[0] // 2, 2 * near
    side = lax.axis_index("zl") if kept else 1 - lax.axis_index("zl")
    square = (count, rows.shape[0])
    out = lax.broadcasted_iota(jnp.int32, square, 0)
    source, rest = out // block, out % block
    place = source * 2 * block + (rest // 2) * 4 + side * 2 + rest % 2
    order = jnp.where(lax.broadcasted_iota(jnp.int32, square, 1) == place, 1.0, 0.0)
    return dot(order.astype(BF16), rows).astype(BF16)


def gated_inner(rows, gate_ref, up_ref):
    return (jax.nn.silu(dot(rows, gate_ref[...])) * dot(rows, up_ref[...])).astype(BF16)


def inner_kernel(rows_ref, g_ref, u_ref, pg_ref, pu_ref, out_ref):
    width = g_ref.shape[1]
    rows = side_rows(rows_ref[...], False)
    out_ref[:, :width] = gated_inner(rows, g_ref, u_ref)
    out_ref[:, width:] = gated_inner(rows, pg_ref, pu_ref)


def own_kernel(rows_ref, g_ref, u_ref, pg_ref, pu_ref, d_ref, pd_ref, out_ref):
    rows = side_rows(rows_ref[...], True)
    out_ref[...] = dot(gated_inner(rows, g_ref, u_ref), d_ref[...]) + dot(
        gated_inner(rows, pg_ref, pu_ref), pd_ref[...]
    )


def down_kernel(own_ref, got_ref, fd_ref, fpd_ref, out_ref):
    width = fd_ref.shape[0]
    got = got_ref[...]
    far = dot(got[:, :width], fd_ref[...]) + dot(got[:, width:], fpd_ref[...])
    out_ref[...] = (own_ref[...] + far).astype(BF16)


def on_device(
    residual, mixer_in, doc_ids, lam_re, lam_im, log_step, log_keep, in_re, in_im, out_re, out_im,
    skip_gain, w_val, w_gate, norm_gain, route_ids, route_wts, exp_gate, exp_up, exp_down,
    shared_gate, shared_up, shared_down,
):
    tok_loc, model_width = residual.shape
    layers = lax.axis_size(Z)
    owners = lax.axis_size(SP)
    top_k = route_ids.shape[1]
    swap = lambda x: lax.ppermute(x, "core", [(0, 1), (1, 0)])
    cross = lambda x: lax.ppermute(x, "zl", [(0, 1), (1, 0)])
    near = lax.axis_size("zh")
    far_val, far_gate = cross(w_val), cross(w_gate)
    gate_w, up_w, down_w = exp_gate[0], exp_up[0], exp_down[0]
    pair_eg, pair_eu, pair_ed = swap(gate_w), swap(up_w), swap(down_w)

    corner = 2 * lax.axis_index("zl") + lax.axis_index("core")
    act_own, act_other = state_mixer(
        mixer_in, doc_ids, lam_re, lam_im, log_step, log_keep, in_re, in_im, out_re, out_im,
        skip_gain,
    )
    act_pair = cross(act_other)
    shape = jax.ShapeDtypeStruct((near, tok_loc, 2 * model_width), BF16)
    kept, sent = call(
        gated_kernel, (shape, shape),
        act_own, act_pair, in_hbm(w_val), in_hbm(w_gate), far_val, far_gate,
    )
    parts = call(sum_kernel, shape, kept, swap(sent))
    parts = lax.all_to_all(parts, "zh", 0, 0, tiled=True)
    capacity = tok_loc * top_k // owners

    def placed(ids, wts, count):
        ids = ids.reshape(count, tok_loc * top_k)
        same = ids[:, :, None] == ids[:, None, :]
        order = jnp.arange(tok_loc * top_k)
        rank = jnp.sum((same & (order[None, :] < order[:, None])).astype(jnp.int32), axis=-1)
        block = count * capacity
        slots = ids * block + capacity * jnp.arange(count, dtype=jnp.int32)[:, None] + rank
        slots = slots.reshape(count * tok_loc, top_k)
        hit = slots[:, :, None] == jnp.arange(owners * block, dtype=jnp.int32)[None, None, :]
        if wts is None:
            return jnp.sum(hit.astype(F32), axis=1).astype(BF16)
        wts = wts.reshape(count * tok_loc, top_k)
        return halves(jnp.sum(jnp.where(hit, wts[:, :, None], 0.0), axis=1))

    def mine(x, count, parts, at):
        x = x.reshape(count, parts, tok_loc, top_k)
        return lax.dynamic_index_in_dim(x, at, 1, keepdims=False)

    block = layers * capacity
    picker = placed(mine(route_ids, layers, 2, lax.axis_index("core")), None, layers)
    weights_high, weights_low = placed(
        mine(route_ids, near, 4, corner), mine(route_wts, near, 4, corner), near
    )
    parts, picker, weights_high, weights_low = lax.optimization_barrier(
        (parts, picker, weights_high, weights_low)
    )
    every, hidden, normed = call(
        norm_kernel,
        (
            jax.ShapeDtypeStruct((layers, tok_loc, model_width), BF16),
            jax.ShapeDtypeStruct(residual.shape, F32),
            jax.ShapeDtypeStruct(residual.shape, BF16),
        ),
        parts, residual, norm_gain.reshape(1, model_width),
    )

    tokens = layers * tok_loc
    every = lax.all_to_all(every, Z, 0, 0, tiled=True).reshape(tokens, model_width)
    base = call(
        shared_kernel, jax.ShapeDtypeStruct(hidden.shape, F32),
        normed, hidden, *map(in_hbm, (shared_gate, shared_up, shared_down)),
    )
    base, down_now = lax.optimization_barrier((base, down_w))
    far_down = cross(down_now)
    every, base = lax.optimization_barrier((every, base))
    far_pair = swap(far_down)
    packed = lax.dot_general(
        picker, every, (((0,), (0,)), ((), ())), preferred_element_type=F32
    ).astype(BF16)
    rows = lax.all_to_all(packed.reshape(owners, block, model_width), SP, 0, 0, tiled=True)
    rows = rows.reshape(owners * block, model_width)
    half = owners * block // 2
    narrow = jax.ShapeDtypeStruct((half, 2 * gate_w.shape[1]), BF16)
    up_pair = tuple(map(in_hbm, (gate_w, up_w, pair_eg, pair_eu)))
    sent = call(inner_kernel, narrow, rows, *up_pair)
    got = cross(sent)
    wide = jax.ShapeDtypeStruct((half, model_width), F32)
    own = call(own_kernel, wide, rows, *up_pair, in_hbm(down_w), in_hbm(pair_ed))
    partial = call(
        down_kernel, jax.ShapeDtypeStruct(wide.shape, BF16), own, got, far_down, far_pair
    )
    back = lax.all_to_all(
        partial.reshape(owners, block // 2, model_width), SP, 0, 0, tiled=True
    ).reshape(half, model_width)
    routed = (dot(weights_high, back) + dot(weights_low, back)).astype(BF16)
    routed = lax.all_to_all(routed.reshape(near, tok_loc, model_width), "zh", 0, 0, tiled=True)
    return (base + jnp.sum(routed.astype(F32), axis=0)).astype(BF16)


def solution(mesh):
    grid = Mesh(mesh.devices.reshape(4, 4, 4, 2, 2), ("y", "x", "zh", "zl", "core"))
    return jax.shard_map(
        on_device,
        mesh=grid,
        in_specs=(
            P(SP + TP, None),
            P(SP, TP),
            P(SP),
            P(TP, None),
            P(TP, None),
            P(TP),
            P(SP, TP),
            P(TP, None, None),
            P(TP, None, None),
            P(TP, None, None),
            P(TP, None, None),
            P(TP),
            P(TP, None),
            P(TP, None),
            P(),
            P(SP, None),
            P(SP, None),
            P(SP, None, TP),
            P(SP, None, TP),
            P(SP, TP, None),
            P(),
            P(),
            P(),
        ),
        out_specs=P(SP + TP, None),
        check_vma=False,
    )
```
